32 devices in a mesh: grp: 2 (over y), sp: 4 (over z), tp: 4 (over x, core).
Axes of the slice: x: 2, y: 2, z: 4, core: 2. Of those that a mesh axis runs over, the one named last changes fastest.
Arguments:
- latents: bfloat16 [3072, 4096], P(('grp', 'sp', 'tp')), parts along dimension 0, may hold values from -3 to 3
- conditions: float32 [4, 4096], P('grp', 'sp'), parts along dimension 0, may hold values from -6 to 6
- context: bfloat16 [1024, 4096], P(('grp', 'sp')), parts along dimension 0, may hold values from -6 to 6
- w_shift: bfloat16 [4096, 4096], P('sp', 'tp'), may hold values from -0.09375 to 0.09375
- w_scale: bfloat16 [4096, 4096], P('sp', 'tp'), may hold values from -0.09375 to 0.09375
- w_gate: bfloat16 [4096, 4096], P('sp', 'tp'), may hold values from -0.09375 to 0.09375
- w_qdown: bfloat16 [4096, 1024], P(None, 'tp'), may hold values from -2 to 2
- w_kvdown: bfloat16 [4096, 512], P(None, 'tp'), may hold values from -2 to 2
- w_rope: bfloat16 [4096, 32], replicated, may hold values from -0.09375 to 0.09375
- q_gain: float32 [1024], replicated, may hold values from 1 to 24
- latent_norm_gain: float32 [512], replicated, may hold values from 0.1 to 1.9
- query_up_weight: bfloat16 [1024, 3072], P(None, 'tp'), may hold values from -0.1875 to 0.1875
- key_up_weight: bfloat16 [512, 2048], P(None, 'tp'), may hold values from -0.25 to 0.25
- value_up_weight: bfloat16 [512, 2048], P(None, 'tp'), may hold values from -0.25 to 0.25
- context_bias: float32 [32], P('tp'), may hold values from 0.5 to 2
- w_out: bfloat16 [2048, 4096], P(None, 'tp'), may hold values from -0.5 to 0.5
Outputs:
- mixed: bfloat16 [3072, 4096], P(('grp', 'sp', 'tp')), parts along dimension 0
The draws below stay inside these ranges and needn't reach their ends.
There are 2 independent parts, one for each index of `grp`. The reference program is written for one: setup_inputs(seed, part) draws one part's arguments, and reference() takes and returns one part's arrays. A program takes and returns all parts, laid end to end along the dimension named above; an argument that names none is the same for every part. Nothing has to cross between parts.
All inputs are finite; a program needn't handle non-finite values.
Results may differ from the reference program's by a relative error of at most 0.01345.
The reference program's roundings to bfloat16 on the way count: a program that leaves them out, or rounds other values in their place, can miss the bound.
Values may be sent and summed in bfloat16 or wider, within the bound.
A program may use at most 64 MiB of HBM per device.

```python
import math
import jax
import jax.numpy as jnp
from jax import lax

MODEL_WIDTH = 4096
HEAD_TOTAL = 32
PLAIN_QK_DIM = 64
ROTARY_DIM = 32
VALUE_DIM = 64
QUERY_RANK = 1024
LATENT_KV_RANK = 512
GRID_W = 64
CTX = 512
TOKENS = 1536


def ascending_columns(key, row_count, col_count):
    entries = jax.random.normal(jax.random.fold_in(key, 11), (row_count, col_count), jnp.float32)
    jitter = jax.random.uniform(jax.random.fold_in(key, 12), (col_count,), jnp.float32, math.log(0.6), math.log(1.6))
    steepness = 10.0
    column_scale = jnp.exp(jitter + math.log(steepness) * jnp.arange(col_count, dtype=jnp.float32) / col_count)
    column_scale = column_scale / jnp.sqrt(jnp.mean(column_scale * column_scale))
    return jnp.clip(jnp.clip(entries, -4.0, 4.0) * column_scale * row_count ** (-0.5), -2.0, 2.0)


def draw_w_qdown(key, part):
    return ascending_columns(jax.random.fold_in(key, 3), MODEL_WIDTH, QUERY_RANK).astype(jnp.bfloat16)


def draw_w_kvdown(key, part):
    return ascending_columns(jax.random.fold_in(key, 5), MODEL_WIDTH, LATENT_KV_RANK).astype(jnp.bfloat16)


def draw_q_gain(key, part):
    return jax.random.uniform(jax.random.fold_in(key, 7), (QUERY_RANK,), jnp.float32, 1.5, 3.5)


def levels(stream_key, shape, shards, smallest, high):
    def one(position, shards_of):
        draws = jax.random.uniform(jax.random.fold_in(jax.random.fold_in(stream_key, 6), position), (shards_of,), jnp.float32, smallest / len(shards), high / len(shards))
        return jnp.repeat(jnp.exp(draws), shape[position] // shards_of).reshape((-1,) + (1,) * (len(shape) - position - 1))

    factor_of = one(*shards[0])
    for cut in shards[1:]:
        factor_of = factor_of * one(*cut)
    return factor_of


def noise(rng, extent, scale, most, cuts=(), held_as=jnp.bfloat16):
    loudness = levels(rng, extent, cuts, -0.22, 0.18) if cuts else 1.0
    result = jax.random.normal(rng, extent, jnp.float32) * scale * loudness
    return jnp.minimum(jnp.maximum(result, -most), most).astype(held_as)


def setup_inputs(seed: int = 0, part: int = 0) -> dict:
    streams_of = jax.random.split(jax.random.key(seed), 17)
    part_splits = jax.random.split(jax.random.fold_in(streams_of[16], part), 17)
    latents = noise(part_splits[0], (TOKENS, MODEL_WIDTH), 0.5, 3.0, ((0, 16),))
    conditions = noise(part_splits[1], (2, MODEL_WIDTH), 1.0, 6.0, ((1, 4),), jnp.float32)
    context = noise(part_splits[2], (CTX, MODEL_WIDTH), 1.0, 6.0, ((0, 4),))
    w_shift = noise(streams_of[3], (MODEL_WIDTH, MODEL_WIDTH), MODEL_WIDTH ** -0.5, 0.09375, ((0, 4), (1, 4)))
    w_scale = noise(streams_of[4], (MODEL_WIDTH, MODEL_WIDTH), MODEL_WIDTH ** -0.5, 0.09375, ((0, 4), (1, 4)))
    w_gate = noise(streams_of[5], (MODEL_WIDTH, MODEL_WIDTH), MODEL_WIDTH ** -0.5, 0.09375, ((0, 4), (1, 4)))
    w_qdown = draw_w_qdown(jax.random.fold_in(streams_of[16], 71), part)
    w_kvdown = draw_w_kvdown(jax.random.fold_in(streams_of[16], 71), part)
    w_rope = noise(streams_of[8], (MODEL_WIDTH, ROTARY_DIM), MODEL_WIDTH ** -0.5, 0.09375)
    q_gain = draw_q_gain(jax.random.fold_in(streams_of[16], 71), part)
    latent_norm_gain = jnp.clip(1.0 + 0.18 * jax.random.normal(streams_of[10], (LATENT_KV_RANK,), jnp.float32), 0.1, 1.9)
    query_up_weight = noise(streams_of[11], (QUERY_RANK, HEAD_TOTAL * (PLAIN_QK_DIM + ROTARY_DIM)), QUERY_RANK ** -0.5, 0.1875, ((1, 4),))
    key_up_weight = noise(streams_of[12], (LATENT_KV_RANK, HEAD_TOTAL * PLAIN_QK_DIM), LATENT_KV_RANK ** -0.5, 0.25, ((1, 4),))
    value_up_weight = noise(streams_of[13], (LATENT_KV_RANK, HEAD_TOTAL * VALUE_DIM), LATENT_KV_RANK ** -0.5, 0.25, ((1, 4),))
    context_bias = jnp.clip(0.5 + 1.5 * jax.random.uniform(streams_of[14], (HEAD_TOTAL,), jnp.float32) ** levels(streams_of[14], (HEAD_TOTAL,), ((0, 4),), -0.2, 0.2), 0.5, 2.0)
    w_out = noise(streams_of[15], (HEAD_TOTAL * VALUE_DIM, MODEL_WIDTH), (HEAD_TOTAL * VALUE_DIM // 16) ** -0.5, 0.5, ((1, 4),))
    return {"latents": latents, "conditions": conditions, "context": context, "w_shift": w_shift, "w_scale": w_scale, "w_gate": w_gate, "w_qdown": w_qdown, "w_kvdown": w_kvdown, "w_rope": w_rope, "q_gain": q_gain, "latent_norm_gain": latent_norm_gain, "query_up_weight": query_up_weight, "key_up_weight": key_up_weight, "value_up_weight": value_up_weight, "context_bias": context_bias, "w_out": w_out}


EPSILON = 1e-06

def layer_modulate(row_block, shift_by, scale_by):
    values = row_block.astype(jnp.float32)
    center = values - lax.optimization_barrier(jnp.mean(values, axis=-1, keepdims=True))
    spread = lax.optimization_barrier(jnp.mean(center * center, axis=-1, keepdims=True))
    normed = center * lax.rsqrt(spread + EPSILON)
    return (normed * (1.0 + scale_by) + shift_by).astype(jnp.bfloat16)

def rms_scale(raw_rows, gain_vec):
    values = raw_rows.astype(jnp.float32)
    factor = lax.rsqrt(lax.optimization_barrier(jnp.mean(values * values, axis=-1, keepdims=True)) + EPSILON)
    return (values * factor * gain_vec).astype(jnp.bfloat16)

def axial_turn(values, positions):
    freq_count = values.shape[-1] // 4
    inverse = 10000.0 ** (-jnp.arange(freq_count, dtype=jnp.float32) / freq_count)
    grid_row = (positions // GRID_W).astype(jnp.float32)
    grid_col = (positions % GRID_W).astype(jnp.float32)
    target = (positions.shape[0],) + (1,) * (values.ndim - 2) + (freq_count,)
    pieces = []
    for half_index, coordinate in enumerate((grid_row, grid_col)):
        angles = (coordinate[:, None] * inverse[None, :]).reshape(target)
        cosine = jnp.cos(angles)
        sine_of = jnp.sin(angles)
        segment = values[..., 2 * half_index * freq_count:2 * (half_index + 1) * freq_count]
        low_half = segment[..., :freq_count]
        high_half = segment[..., freq_count:]
        pieces.append(low_half * cosine - high_half * sine_of)
        pieces.append(low_half * sine_of + high_half * cosine)
    return jnp.concatenate(pieces, axis=-1)

def reference(latents, conditions, context, w_shift, w_scale, w_gate, w_qdown, w_kvdown, w_rope, q_gain, latent_norm_gain, query_up_weight, key_up_weight, value_up_weight, context_bias, w_out):
    cond_act = jax.nn.silu(conditions.astype(jnp.float32)).astype(jnp.bfloat16)
    shift_lat = jnp.dot(cond_act[0], w_shift, preferred_element_type=jnp.float32)
    scale_lat = jnp.dot(cond_act[0], w_scale, preferred_element_type=jnp.float32)
    gate_lat = jnp.dot(cond_act[0], w_gate, preferred_element_type=jnp.float32)
    shift_ctx = jnp.dot(cond_act[1], w_shift, preferred_element_type=jnp.float32)
    scale_ctx = jnp.dot(cond_act[1], w_scale, preferred_element_type=jnp.float32)
    h_lat = layer_modulate(latents, shift_lat, scale_lat)
    h_ctx = layer_modulate(context, shift_ctx, scale_ctx)
    cq_all = rms_scale(jnp.dot(h_lat, w_qdown, preferred_element_type=jnp.float32).astype(jnp.bfloat16), q_gain)
    ckv_lat = rms_scale(jnp.dot(h_lat, w_kvdown, preferred_element_type=jnp.float32).astype(jnp.bfloat16), latent_norm_gain)
    ckv_ctx = rms_scale(jnp.dot(h_ctx, w_kvdown, preferred_element_type=jnp.float32).astype(jnp.bfloat16), latent_norm_gain)
    positions = jnp.arange(TOKENS, dtype=jnp.int32)
    kr_lat = axial_turn(jnp.dot(h_lat, w_rope, preferred_element_type=jnp.float32), positions).astype(jnp.bfloat16)
    kr_ctx = jnp.dot(h_ctx, w_rope, preferred_element_type=jnp.float32).astype(jnp.bfloat16)
    q_all = jnp.dot(cq_all, query_up_weight, preferred_element_type=jnp.float32).reshape(TOKENS, HEAD_TOTAL, PLAIN_QK_DIM + ROTARY_DIM)
    queries = jnp.concatenate([q_all[..., :PLAIN_QK_DIM], axial_turn(q_all[..., PLAIN_QK_DIM:], positions)], axis=-1).astype(jnp.bfloat16)
    key_rows = jnp.concatenate([jnp.dot(ckv_lat, key_up_weight, preferred_element_type=jnp.float32).astype(jnp.bfloat16), jnp.dot(ckv_ctx, key_up_weight, preferred_element_type=jnp.float32).astype(jnp.bfloat16)], axis=0)
    value_rows = jnp.concatenate([jnp.dot(ckv_lat, value_up_weight, preferred_element_type=jnp.float32).astype(jnp.bfloat16), jnp.dot(ckv_ctx, value_up_weight, preferred_element_type=jnp.float32).astype(jnp.bfloat16)], axis=0)
    key_rows = key_rows.reshape(TOKENS + CTX, HEAD_TOTAL, PLAIN_QK_DIM)
    value_rows = value_rows.reshape(TOKENS + CTX, HEAD_TOTAL, VALUE_DIM)
    rope_keys = jnp.concatenate([kr_lat, kr_ctx], axis=0)
    is_ctx = (jnp.arange(TOKENS + CTX, dtype=jnp.int32) >= TOKENS).astype(jnp.float32)
    score_scale = (PLAIN_QK_DIM + ROTARY_DIM) ** (-0.5)

    def one_head(operands):
        head_q, head_k, head_v, head_bias = operands
        scores = jnp.dot(head_q[:, :PLAIN_QK_DIM], head_k.T, preferred_element_type=jnp.float32)
        scores = scores + jnp.dot(head_q[:, PLAIN_QK_DIM:], rope_keys.T, preferred_element_type=jnp.float32)
        scores = scores * score_scale + head_bias * is_ctx[None, :]
        largest = lax.optimization_barrier(jnp.max(scores, axis=-1, keepdims=True))
        exponent = jnp.exp(scores - largest)
        row_sum = lax.optimization_barrier(jnp.sum(exponent, axis=-1, keepdims=True))
        weights = exponent.astype(jnp.bfloat16)
        return (jnp.dot(weights, head_v, preferred_element_type=jnp.float32) / row_sum).astype(jnp.bfloat16)
    attended = lax.map(one_head, (queries.transpose(1, 0, 2), key_rows.transpose(1, 0, 2), value_rows.transpose(1, 0, 2), context_bias))
    attended = attended.transpose(1, 0, 2).reshape(TOKENS, HEAD_TOTAL * VALUE_DIM)
    projected = jnp.dot(attended, w_out, preferred_element_type=jnp.float32).astype(jnp.bfloat16)
    return (latents.astype(jnp.float32) + gate_lat * projected.astype(jnp.float32)).astype(jnp.bfloat16)
```

```python
import functools

import jax
import jax.numpy as jnp
import numpy as np
from jax import lax
from jax.experimental import pallas as pl
from jax.experimental.pallas import tpu as pltpu
from jax.sharding import PartitionSpec as P

PLAIN_QK_DIM = 64
ROTARY_DIM = 32
VALUE_DIM = 64
GRID_W = 64


EPSILON = 1e-06
NEGATIVE = -1e30


def layer_modulate(row_block, shift_by, scale_by):
    values = row_block.astype(jnp.float32)
    center = values - jnp.mean(values, axis=-1, keepdims=True)
    spread = jnp.mean(center * center, axis=-1, keepdims=True)
    normed = center * lax.rsqrt(spread + EPSILON)
    return (normed * (1.0 + scale_by) + shift_by).astype(jnp.bfloat16)


def rms_scale(raw_rows, gain_vec):
    values = raw_rows.astype(jnp.float32)
    factor = lax.rsqrt(jnp.mean(values * values, axis=-1, keepdims=True) + EPSILON)
    return (values * factor * gain_vec).astype(jnp.bfloat16)


def axial_turn(values, positions):
    freq_count = values.shape[-1] // 4
    inverse = 10000.0 ** (-jnp.arange(freq_count, dtype=jnp.float32) / freq_count)
    grid_row = (positions // GRID_W).astype(jnp.float32)
    grid_col = (positions % GRID_W).astype(jnp.float32)
    target = (positions.shape[0],) + (1,) * (values.ndim - 2) + (freq_count,)
    pieces = []
    for half_index, coordinate in enumerate((grid_row, grid_col)):
        angles = (coordinate[:, None] * inverse[None, :]).reshape(target)
        cosine = jnp.cos(angles)
        sine_of = jnp.sin(angles)
        segment = values[..., 2 * half_index * freq_count : 2 * (half_index + 1) * freq_count]
        low_half = segment[..., :freq_count]
        high_half = segment[..., freq_count:]
        pieces.append(low_half * cosine - high_half * sine_of)
        pieces.append(low_half * sine_of + high_half * cosine)
    return jnp.concatenate(pieces, axis=-1)


def plain_device(
    latents,
    conditions,
    context,
    w_shift,
    w_scale,
    w_gate,
    w_qdown,
    w_kvdown,
    w_rope,
    q_gain,
    latent_norm_gain,
    query_up_weight,
    key_up_weight,
    value_up_weight,
    context_bias,
    w_out,
):
    tp_count = lax.axis_size("tp")
    tp_index = lax.axis_index("tp")
    sp_index = lax.axis_index("sp")
    own_rows = latents.shape[0]
    tok_count = own_rows * tp_count
    ctx_share = context.shape[0] // tp_count
    cond_act = jax.nn.silu(conditions).astype(jnp.bfloat16)
    partial_mod = jnp.concatenate(
        [
            jnp.dot(cond_act, w_shift, preferred_element_type=jnp.float32),
            jnp.dot(cond_act, w_scale, preferred_element_type=jnp.float32),
            jnp.dot(cond_act[0:1], w_gate, preferred_element_type=jnp.float32),
        ],
        axis=0,
    )
    summed = lax.psum(partial_mod, "sp")
    modulation = lax.all_gather(summed, "tp", axis=1, tiled=True)
    ctx_own = lax.dynamic_slice_in_dim(context, tp_index * ctx_share, ctx_share, 0)
    h_lat = layer_modulate(latents, modulation[0], modulation[2])
    h_ctx = layer_modulate(ctx_own, modulation[1], modulation[3])
    h_own = jnp.concatenate([h_lat, h_ctx], axis=0)
    rope_raw = jnp.dot(h_own, w_rope, preferred_element_type=jnp.float32)
    own_pos = sp_index * tok_count + tp_index * own_rows + jnp.arange(own_rows, dtype=jnp.int32)
    kr_lat = axial_turn(rope_raw[:own_rows], own_pos).astype(jnp.bfloat16)
    kr_ctx = rope_raw[own_rows:].astype(jnp.bfloat16)
    arrived = lax.all_gather(h_own, "tp", axis=0, tiled=True)
    projected = jnp.concatenate(
        [
            jnp.dot(arrived, w_qdown, preferred_element_type=jnp.float32),
            jnp.dot(arrived, w_kvdown, preferred_element_type=jnp.float32),
        ],
        axis=1,
    ).astype(jnp.bfloat16)
    q_cols = w_qdown.shape[1]
    grouped = projected.reshape(tp_count, own_rows + ctx_share, projected.shape[1])
    cq_cols = grouped[:, :own_rows, :q_cols].reshape(tok_count, q_cols)
    kvl_cols = grouped[:, :own_rows, q_cols:].reshape(tok_count, w_kvdown.shape[1])
    kvc_cols = grouped[:, own_rows:, q_cols:].reshape(tp_count * ctx_share, w_kvdown.shape[1])
    cq_raw, kvl_raw, kvc_raw, krl_all, krc_all = (
        lax.all_gather(cq_cols, "tp", axis=1, tiled=True),
        lax.all_gather(kvl_cols, "tp", axis=1, tiled=True),
        lax.all_gather(kvc_cols, "tp", axis=1, tiled=True),
        lax.all_gather(kr_lat, "tp", axis=0, tiled=True),
        lax.all_gather(kr_ctx, "tp", axis=0, tiled=True),
    )
    cq_all = rms_scale(cq_raw, q_gain)
    ckv_all = jnp.concatenate(
        [rms_scale(kvl_raw, latent_norm_gain), rms_scale(kvc_raw, latent_norm_gain)], axis=0
    )
    kr_all = jnp.concatenate([krl_all, krc_all], axis=0)
    head_count = query_up_weight.shape[1] // (PLAIN_QK_DIM + ROTARY_DIM)
    q_all = jnp.dot(cq_all, query_up_weight, preferred_element_type=jnp.float32)
    q_all = q_all.reshape(tok_count, head_count, PLAIN_QK_DIM + ROTARY_DIM)
    query_pos = sp_index * tok_count + jnp.arange(tok_count, dtype=jnp.int32)
    queries = jnp.concatenate(
        [q_all[..., :PLAIN_QK_DIM], axial_turn(q_all[..., PLAIN_QK_DIM:], query_pos)], axis=-1
    ).astype(jnp.bfloat16)
    q_nope = queries[..., :PLAIN_QK_DIM]
    q_rope = queries[..., PLAIN_QK_DIM:]
    seg_rows = ckv_all.shape[0]
    is_ctx = (jnp.arange(seg_rows, dtype=jnp.int32) >= tok_count).astype(jnp.float32)
    bias_row = context_bias[None, :, None] * is_ctx[None, None, :]
    score_scale = (PLAIN_QK_DIM + ROTARY_DIM) ** (-0.5)

    def attend_block(running, key_block, value_block, rope_block):
        running_max, running_sum, numerator = running
        scores = jnp.einsum("ihd,jhd->ihj", q_nope, key_block, preferred_element_type=jnp.float32)
        scores = scores + jnp.einsum(
            "ihd,jd->ihj", q_rope, rope_block, preferred_element_type=jnp.float32
        )
        scores = scores * score_scale + bias_row
        new_max = jnp.maximum(running_max, jnp.max(scores, axis=-1))
        rescale = jnp.exp(running_max - new_max)
        exponent = jnp.exp(scores - new_max[..., None])
        running_sum = running_sum * rescale + jnp.sum(exponent, axis=-1)
        numerator = numerator * rescale[..., None] + jnp.einsum(
            "ihj,jhd->ihd",
            exponent.astype(jnp.bfloat16),
            value_block,
            preferred_element_type=jnp.float32,
        )
        return (new_max, running_sum, numerator)

    initial = (
        jnp.full((tok_count, head_count), NEGATIVE, jnp.float32),
        jnp.zeros((tok_count, head_count), jnp.float32),
        jnp.zeros((tok_count, head_count, VALUE_DIM), jnp.float32),
    )

    def expand_latent(key_group):
        latent_rows, rope_block = key_group
        key_block = jnp.dot(latent_rows, key_up_weight, preferred_element_type=jnp.float32).astype(
            jnp.bfloat16
        )
        value_block = jnp.dot(
            latent_rows, value_up_weight, preferred_element_type=jnp.float32
        ).astype(jnp.bfloat16)
        return (
            key_block.reshape(seg_rows, head_count, PLAIN_QK_DIM),
            value_block.reshape(seg_rows, head_count, VALUE_DIM),
            rope_block,
        )

    members = (
        lax.all_gather(ckv_all, "sp", axis=0, tiled=True),
        lax.all_gather(kr_all, "sp", axis=0, tiled=True),
    )
    block_count = members[0].shape[0] // seg_rows
    stacked = tuple(
        (member.reshape((block_count, seg_rows) + member.shape[1:]) for member in members)
    )

    def step_fn(state, key_group):
        key_block, value_block, rope_block = expand_latent(key_group)
        return (attend_block(state, key_block, value_block, rope_block), None)

    result, unused = lax.scan(step_fn, initial, stacked)
    running_max, running_sum, numerator = result
    attended = (
        (numerator / running_sum[..., None])
        .astype(jnp.bfloat16)
        .reshape(tok_count, head_count * VALUE_DIM)
    )
    proj_cols = jnp.dot(
        lax.all_gather(attended, "tp", axis=1, tiled=True),
        w_out,
        preferred_element_type=jnp.float32,
    )
    proj_rows = lax.all_to_all(
        proj_cols.astype(jnp.bfloat16), "tp", split_axis=0, concat_axis=1, tiled=True
    )
    mixed_rows = latents.astype(jnp.float32) + modulation[4] * proj_rows.astype(jnp.float32)
    return mixed_rows.astype(jnp.bfloat16)


MESH = pl.DeviceIdType.MESH
LOG2E = 1.4426950408889634
STEP = 16
BAND = 32


def turn_tables(blocks, own):
    freq_count = ROTARY_DIM // 4
    inverse = 10000.0 ** (-np.arange(freq_count) / freq_count)
    tokens = blocks * 4 * own
    position = np.arange(tokens).reshape(blocks, 4, 2, own // 2).swapaxes(1, 2).reshape(-1)
    cosine = np.zeros((tokens, 128), np.float32)
    sine = np.zeros((tokens, 128), np.float32)
    cosine[:, :PLAIN_QK_DIM] = 1.0
    for half_index, coordinate in enumerate((position // GRID_W, position % GRID_W)):
        angles = coordinate[:, None] * inverse[None, :]
        low = PLAIN_QK_DIM + 2 * half_index * freq_count
        high = low + freq_count
        cosine[:, low : low + freq_count] = np.cos(angles)
        cosine[:, high : high + freq_count] = np.cos(angles)
        sine[:, low : low + freq_count] = -np.sin(angles)
        sine[:, high : high + freq_count] = np.sin(angles)
    return cosine, sine


def lanes_of(shape):
    return lax.broadcasted_iota(jnp.int32, shape, len(shape) - 1)


def turned(values, cosine, sine):
    lane = lanes_of(values.shape)
    swapped = jnp.where(
        (lane // 8) % 2 == 0, pltpu.roll(values, 120, 1), pltpu.roll(values, 8, 1)
    )
    return values * cosine + swapped * sine


def block_kernel(
    cond_hbm,
    bias_hbm,
    qgain_hbm,
    kvgain_hbm,
    rope_hbm,
    lat_hbm,
    ctx_hbm,
    wsh_hbm,
    wsc_hbm,
    wga_hbm,
    wqd_hbm,
    wkd_hbm,
    wqu_hbm,
    wku_hbm,
    wvu_hbm,
    wo_hbm,
    cos_hbm,
    sin_hbm,
    out_hbm,
    cond_ref,
    bias_ref,
    qgain_ref,
    kvgain_ref,
    rope_ref,
    cond16,
    w3,
    lat,
    ctx,
    hid,
    wqd,
    wkvr,
    modp,
    mod,
    cq,
    kvx,
    krx,
    kraw,
    ckn,
    cqn,
    wqu,
    wku,
    wvu,
    wo,
    cosv,
    sinv,
    qh,
    kb,
    vb,
    acc,
    mx,
    att,
    po,
    pr,
    st_mean,
    st_rate,
    part_self,
    part_other,
    outv,
    load_sem,
    send_sem,
    recv_sem,
    zsend,
    zrecv,
    ssend,
    srecv,
    out_sem,
):
    f32, bf16 = jnp.float32, jnp.bfloat16
    spn = lax.axis_size("sp")
    p = lax.axis_index("tp")
    z = lax.axis_index("sp")
    core = lax.rem(p, 2)
    side = p // 2
    p1, p2, p3 = p ^ 1, p ^ 2, p ^ 3
    own = lat.shape[1]
    width = lat.shape[2]
    half = own // 2
    tok = own * 4
    pair = own * 2
    ctxn = ctx.shape[0]
    seg = tok + ctxn
    arows = ctxn + pair
    modw = w3.shape[2]
    heads = qh.shape[0]
    kcols = kvx.shape[3]
    spans = ((0, arows), (arows, pair))

    loads = []

    def load(src, dst):
        copy = pltpu.make_async_copy(src, dst, load_sem.at[len(loads)])
        loads.append(copy)
        copy.start()
        return copy

    l_lat = load(lat_hbm, lat.at[p])
    l_cond = load(cond_hbm, cond_ref)
    l_rope = load(rope_hbm, rope_ref)
    l_w3 = [load(ref, w3.at[i]) for i, ref in enumerate((wsh_hbm, wsc_hbm, wga_hbm))]
    l_ctx = load(ctx_hbm, ctx)
    l_kd = load(wkd_hbm, wkvr.at[:, pl.ds(0, kcols)])
    l_qd = load(wqd_hbm, wqd)
    table_rows = pl.ds(pl.multiple_of(z * tok, 8), tok)
    l_cos = load(cos_hbm.at[table_rows], cosv)
    l_sin = load(sin_hbm.at[table_rows], sinv)
    l_ku = load(wku_hbm, wku)
    l_vu = load(wvu_hbm, wvu)
    l_qu = load(wqu_hbm, wqu)
    l_wo = load(wo_hbm, wo)
    l_small = [
        load(bias_hbm, bias_ref),
        load(qgain_hbm, qgain_ref),
        load(kvgain_hbm, kvgain_ref),
    ]

    barrier = pltpu.get_barrier_semaphore()
    for peer in (p1, p2, p3):
        pl.semaphore_signal(barrier, inc=1, device_id={"tp": peer}, device_id_type=MESH)
    for d in range(1, spn):
        pl.semaphore_signal(
            barrier, inc=1, device_id={"sp": lax.rem(z + d, spn)}, device_id_type=MESH
        )

    sends = []

    def copy_to(src, dst, s_sem, r_sem, target):
        return pltpu.make_async_remote_copy(
            src_ref=src,
            dst_ref=dst,
            send_sem=s_sem,
            recv_sem=r_sem,
            device_id=target,
            device_id_type=MESH,
        )

    def send(src, dst, index, target):
        copy = copy_to(src, dst, send_sem.at[index], recv_sem.at[index], target)
        copy.start()
        sends.append(copy)
        return copy

    counter = [0]

    def fresh():
        counter[0] += 1
        return counter[0] - 1

    def near(view):
        return send(view(p), view(p), fresh(), {"tp": p1}).wait_recv

    def far(view, far_view=None):
        far_view = far_view or view
        i2, i3 = fresh(), fresh()
        first = send(view(p), view(p), i2, {"tp": p2})

        def relay():
            first.wait_recv()
            return send(far_view(p2), far_view(p2), i3, {"tp": p1}).wait_recv

        return relay

    l_cond.wait()
    cond16[...] = jnp.zeros_like(cond16)
    cond16[0:2, :] = cond_ref[...]
    conditions = cond16[...]
    act = (conditions / (1.0 + jnp.exp(-conditions))).astype(bf16)
    l_rope.wait()
    for c in range(0, width, 128):
        wkvr[c : c + 128, kcols:] = jnp.concatenate(
            [
                jnp.swapaxes(rope_ref[:, c : c + 128].astype(f32), 0, 1).astype(bf16),
                jnp.zeros((128, wkvr.shape[1] - kcols - ROTARY_DIM), bf16),
            ],
            axis=1,
        )

    pl.semaphore_wait(barrier, 3 + spn - 1)

    l_lat.wait()
    pieces_a = [(0, BAND), (BAND, half - BAND)]
    pieces_b = [(half, BAND), (half + BAND, half - BAND)]

    def piece_of(r, n):
        return lambda slot: lat.at[slot, pl.ds(r, n)]

    relay_lat = [far(piece_of(*pieces_a[0]))]
    lat_near = near(lambda slot: lat.at[slot])

    for i in range(3):
        l_w3[i].wait()
        partial_mod = jnp.dot(act, w3[i], preferred_element_type=f32)
        modp[z, 2 * i : 2 * i + 2, :] = partial_mod[0:2]
    modp[z, 6:8, :] = jnp.zeros((2, modw), f32)
    mod_waits = []
    for d in range(1, spn):
        mod_waits.append(
            send(modp.at[z], modp.at[z], fresh(), {"sp": lax.rem(z + d, spn)})
        )

    def measured(src, row_count, dst_row, step=BAND):
        @pl.loop(0, row_count // step)
        def _(i):
            rows = pl.ds(pl.multiple_of(i * step, STEP), step)
            to = pl.ds(pl.multiple_of(dst_row + i * step, STEP), step)
            tiles = [slice(c, c + 128) for c in range(0, width, 128)]
            sums = jnp.zeros((step, 128), f32)
            for c in tiles:
                sums = sums + src[rows, c].astype(f32)
            mean = jnp.broadcast_to(
                jnp.sum(sums, axis=-1, keepdims=True) * (1.0 / width), (step, 128)
            )
            squares = jnp.zeros((step, 128), f32)
            for c in tiles:
                center = src[rows, c].astype(f32) - mean
                squares = squares + center * center
            spread_of = jnp.sum(squares, axis=-1, keepdims=True) * (1.0 / width)
            st_mean[to, :] = mean
            st_rate[to, :] = jnp.broadcast_to(lax.rsqrt(spread_of + EPSILON), (step, 128))

    def modulate(src, row_count, dst_row, which, step=BAND):
        @pl.loop(0, row_count // step)
        def _(i):
            rows = pl.ds(pl.multiple_of(i * step, STEP), step)
            to = pl.ds(pl.multiple_of(dst_row + i * step, STEP), step)
            mean, rate = st_mean[to, :], st_rate[to, :]
            for c in range(0, width, 128):
                j, k = c // modw, c % modw
                shift_by = mod[j, which : which + 1, k : k + 128]
                scale_by = mod[j, 2 + which : 3 + which, k : k + 128]
                normed = (src[rows, c : c + 128].astype(f32) - mean) * rate
                hid[to, c : c + 128] = (normed * (1.0 + scale_by) + shift_by).astype(bf16)

    def hid_row(dev, r):
        return ctxn + (r // half) * pair + dev * half + r % half

    def band_view(dev, b):
        return lat.at[dev, pl.ds(b * half, half)]

    def take(dev, piece):
        r, n = piece
        measured(lat.at[dev, pl.ds(r, n)], n, hid_row(dev, r), n)
        modulate(lat.at[dev, pl.ds(r, n)], n, hid_row(dev, r), 0, n)

    for b in range(2):
        measured(band_view(p, b), half, hid_row(p, b * half), STEP)
    l_ctx.wait()
    measured(ctx, ctxn, 0)
    for copy in mod_waits:
        copy.wait_recv()
    total = modp[0]
    for i in range(1, spn):
        total = total + modp[i]
    mod[p] = total
    mod_waits = [send(mod.at[p], mod.at[p], fresh(), {"tp": peer}) for peer in (p2, p3, p1)]
    for piece in pieces_a[1:] + pieces_b:
        relay_lat.append(far(piece_of(*piece)))
    lat_near()
    for b in range(2):
        measured(band_view(p1, b), half, hid_row(p1, b * half), STEP)
    lat_far = [relay_lat[0]()]
    for copy in mod_waits:
        copy.wait_recv()
    modulate(ctx, ctxn, 0, 1)
    for dev in (p, p1):
        modulate(band_view(dev, 0), half, hid_row(dev, 0), 0, STEP)
    take(p2, pieces_a[0])
    lat_far.append(relay_lat[1]())
    take(p2, pieces_a[1])
    for n, piece in enumerate(pieces_a):
        lat_far[n]()
        take(p3, piece)

    def kv_piece(o, slot, part):
        first, count = spans[part]
        return kvx.at[o, slot, pl.ds(first, count)]

    def kr_piece(o, part):
        first, count = spans[part]
        return krx.at[o, pl.ds(first // 4, count // 4)]

    class Hop:
        def __init__(self, origin, target, way, part):
            views = (kv_piece(origin, p, part), kr_piece(origin, part))
            self.copies = [
                copy_to(
                    view,
                    view,
                    zsend.at[way, part, kind, origin],
                    zrecv.at[part, kind, origin],
                    {"sp": target},
                )
                for kind, view in enumerate(views)
            ]

        def start(self):
            for copy in self.copies:
                copy.start()

        def wait_recv(self):
            for copy in self.copies:
                copy.wait_recv()

        def wait_send(self):
            for copy in self.copies:
                copy.wait_send()

    def swap(o, part, kind):
        view = kv_piece(o, p2 if kind == 2 else p, part)
        target = p2 if kind == 0 else p1
        return copy_to(
            view, view, ssend.at[kind, part, o], srecv.at[kind, part, o], {"tp": target}
        )

    has_right = z + 1 < spn
    has_left = z >= 1

    def spread(o, part):
        swap(o, part, 0).start()
        swap(o, part, 1).start()

    def relay(o, part):
        swap(o, part, 0).wait_recv()
        swap(o, part, 2).start()

    def gathered(o, part):
        swap(o, part, 1).wait_recv()
        swap(o, part, 2).wait_recv()

    def at_distance(step, fn):
        left, right = z - 1 - step, z + 1 + step

        @pl.when(left >= 0)
        def _():
            fn(left, 0, z + 1, has_right)

        @pl.when(right < spn)
        def _():
            fn(right, 1, z - 1, has_left)

    def forward(step, part):
        def one(o, way, onward, more):
            Hop(o, z, way, part).wait_recv()

            @pl.when(more)
            def _():
                Hop(o, onward, way, part).start()

        at_distance(step, one)

    def spread_at(step, part):
        at_distance(step, lambda o, way, onward, more: spread(o, part))

    def down(part):
        first, count = spans[part]
        both = jnp.dot(hid[first : first + count, :], wkvr[...], preferred_element_type=f32)
        kvx[z, p, first : first + count, :] = both[:, :kcols].astype(bf16)
        kraw[first : first + count, :] = pltpu.roll(both[:, kcols:], 64, 1)
        low = max(first, ctxn)
        tabled = slice(low - ctxn, first + count - ctxn)
        kraw[low : first + count, :] = turned(
            kraw[low : first + count, :], cosv[tabled, :], sinv[tabled, :]
        )
        for t in range(first // 64, (first + count) // 64):
            packed = None
            for j in range(4):
                row = 64 * t + j * STEP
                moved = pltpu.roll(kraw[row : row + STEP, :], (32 * j + 64) % 128, 1)
                packed = moved if packed is None else packed + moved
            krx[z, STEP * t : STEP * t + STEP, :] = packed.astype(bf16)
        spread(z, part)

        @pl.when(has_right)
        def _():
            Hop(z, z + 1, 0, part).start()

        @pl.when(has_left)
        def _():
            Hop(z, z - 1, 1, part).start()

        rows = slice(low, first + count)
        cq[p, part] = jnp.dot(hid[rows, :], wqd[...], preferred_element_type=f32).astype(bf16)
        view = lambda slot: cq.at[slot, part]
        return far(view), near(view)

    l_kd.wait()
    l_qd.wait()
    l_cos.wait()
    l_sin.wait()
    cq_a = down(0)
    for dev in (p, p1):
        modulate(band_view(dev, 1), half, hid_row(dev, half), 0, STEP)
    for n, piece in enumerate(pieces_b):
        lat_far.append(relay_lat[2 + n]())
        take(p2, piece)
    forward(0, 0)
    for n, piece in enumerate(pieces_b):
        lat_far[2 + n]()
        take(p3, piece)
    relay(z, 0)
    forward(1, 0)
    cq_b = down(1)
    spread_at(0, 0)
    cq_waits = [cq_a[1], cq_b[1], cq_a[0]()]
    forward(0, 1)
    spread_at(0, 1)
    relay(z, 1)
    forward(2, 0)
    spread_at(1, 0)

    def rms(pieces, gain_ref, store):
        values = [piece.astype(f32) for piece in pieces]
        total_of = None
        for v in values:
            s = jnp.sum(v * v, axis=-1, keepdims=True)
            total_of = s if total_of is None else total_of + s
        cols = values[0].shape[1]
        factor = lax.rsqrt(total_of / (cols * len(values)) + EPSILON)
        for j, v in enumerate(values):
            gain = gain_ref[0:1, j * cols : (j + 1) * cols]
            store(slice(j * cols, (j + 1) * cols), (v * factor * gain).astype(bf16))

    def expand(block):
        for base in range(0, seg, 64):
            def put(cols, value, base=base):
                ckn[base : base + 64, cols] = value

            rms([kvx[block, r, base : base + 64, :] for r in range(4)], kvgain_ref, put)
        hrow = seg // 2
        lane_h = lanes_of((hrow, 128))
        ones = (lane_h == VALUE_DIM).astype(f32)
        lane_s = lanes_of((STEP, 128))
        on_rope = (lane_s >= PLAIN_QK_DIM) & (lane_s < PLAIN_QK_DIM + ROTARY_DIM)
        for hf in range(2):
            rows = slice(hf * hrow, (hf + 1) * hrow)
            latent_rows = ckn[rows, :]
            pieces = []
            for t in range(4 * hf, 4 * hf + 4):
                packed = krx[block, STEP * t : STEP * t + STEP, :].astype(f32)
                for j in range(4):
                    moved = pltpu.roll(packed, (192 - 32 * j) % 128, 1)
                    pieces.append(jnp.where(on_rope, moved, 0.0))
            rope_key = jnp.concatenate(pieces, axis=0)
            keys = jnp.dot(latent_rows, wku[...], preferred_element_type=f32)
            vals = jnp.dot(latent_rows, wvu[...], preferred_element_type=f32)
            for hp in range(heads // 2):
                cols = slice(128 * hp, 128 * hp + 128)
                k2, v2 = keys[:, cols], vals[:, cols]
                kb[2 * hp, rows, :] = jnp.where(lane_h < 64, k2, rope_key).astype(bf16)
                kb[2 * hp + 1, rows, :] = jnp.where(
                    lane_h < 64, pltpu.roll(k2, 64, 1), rope_key
                ).astype(bf16)
                vb[2 * hp, rows, :] = jnp.where(lane_h < 64, v2, ones).astype(bf16)
                vb[2 * hp + 1, rows, :] = jnp.where(
                    lane_h < 64, pltpu.roll(v2, 64, 1), ones
                ).astype(bf16)

    for copy in l_small:
        copy.wait()
    l_ku.wait()
    l_vu.wait()
    for part in range(2):
        gathered(z, part)
    forward(1, 1)
    spread_at(1, 1)
    cq_waits.append(cq_b[0]())
    spread_at(2, 0)
    expand(z)
    acc[...] = jnp.zeros_like(acc)
    mx[...] = jnp.full(mx.shape, NEGATIVE, f32)
    factor = (PLAIN_QK_DIM + ROTARY_DIM) ** (-0.5) * LOG2E

    for w in cq_waits:
        w()
    for base in range(0, tok, 64):
        def put(cols, value, base=base):
            cqn[base : base + 64, cols] = value

        rms(
            [cq[r, base // pair, base % pair : base % pair + 64, :] for r in range(4)],
            qgain_ref,
            put,
        )
    l_qu.wait()
    q_all = jnp.dot(cqn[...], wqu[...], preferred_element_type=f32)
    lane = lanes_of((tok, 128))
    for h in range(heads):
        offset = h * (PLAIN_QK_DIM + ROTARY_DIM)
        tile, shift = offset // 128, offset % 128
        head = q_all[:, 128 * tile : 128 * tile + 128]
        if shift:
            head = pltpu.roll(head, 128 - shift, 1)
            if shift + PLAIN_QK_DIM + ROTARY_DIM > 128:
                rest = pltpu.roll(q_all[:, 128 * tile + 128 : 128 * tile + 256], 128 - shift, 1)
                head = jnp.where(lane < 128 - shift, head, rest)
        qh[h] = turned(head, cosv[...], sinv[...]).astype(bf16)
    forward(2, 1)
    spread_at(2, 1)

    def score(h):
        return lax.dot_general(
            qh[h], kb[h], (((1,), (1,)), ((), ())), preferred_element_type=f32
        )

    def attend(h, scores):
        tiles = [scores[:, c : c + 128] * factor for c in range(0, seg, 128)]
        bias = bias_ref[h] * LOG2E
        tiles = [t + bias if n * 128 < ctxn else t for n, t in enumerate(tiles)]
        best = functools.reduce(jnp.maximum, tiles)
        old = mx[h]
        new = jnp.maximum(old, jnp.max(best, axis=-1, keepdims=True))
        mx[h] = new
        weights = jnp.concatenate([jnp.exp2(t - new).astype(bf16) for t in tiles], axis=1)
        acc[h] = acc[h] * jnp.exp2(old - new) + jnp.dot(
            weights, vb[h], preferred_element_type=f32
        )

    def attend_all(after):
        scores = score(0)
        for h in range(heads):
            following = score(h + 1) if h + 1 < heads else None
            attend(h, scores)
            after(h)
            scores = following

    def block_at(step):
        below = jnp.minimum(z, spn - 1 - z)
        near_block = jnp.where(lax.rem(step, 2) == 1, z - (step + 1) // 2, z + step // 2)
        past = jnp.where(z < spn - 1 - z, step, spn - 1 - step)
        return jnp.where(step <= 2 * below, near_block, past)

    relay(block_at(jnp.int32(1)), 0)
    relay(block_at(jnp.int32(1)), 1)

    @pl.loop(1, spn)
    def _(step):
        attend_all(lambda h: None)
        block = block_at(step)

        @pl.when(step + 1 < spn)
        def _():
            later = block_at(step + 1)
            relay(later, 0)
            relay(later, 1)

        for part in range(2):
            gathered(block, part)
        expand(block)

    att_relay, att_near = [], []
    lane64 = lane < 64
    quarter = own

    def finish(h):
        if h % 2 == 0:
            return
        hp = h // 2
        outs = []
        for g in (h - 1, h):
            a = acc[g]
            outs.append(a / a[:, VALUE_DIM : VALUE_DIM + 1])
        value = jnp.where(lane64, outs[0], pltpu.roll(outs[1], 64, 1)).astype(bf16)
        for b in range(2):
            for s in range(2):
                row = (2 * b + s) * quarter
                att[p, hp, b, s] = value[row : row + quarter]
        att_relay.append(
            far(
                lambda slot: att.at[slot, hp, :, side],
                lambda slot: att.at[slot, hp, :, 1 - side],
            )
        )
        att_near.append(near(lambda slot: att.at[slot, hp]))

    attend_all(finish)

    hps = heads // 2
    for first in range(0, hps, 2):
        att_relay.append(
            far(
                lambda slot, first=first: att.at[slot, pl.ds(first, 2), :, 1 - side],
                lambda slot, first=first: att.at[slot, pl.ds(first, 2), :, side],
            )
        )
    l_wo.wait()
    half_k = heads * VALUE_DIM * 2

    def project(rows_side, chip):
        joined = jnp.concatenate(
            [
                jnp.concatenate([att[2 * chip + r, hp, b, rows_side] for b in range(2)], axis=0)
                for r in range(2)
                for hp in range(hps)
            ],
            axis=1,
        )
        k_rows = pl.ds(pl.multiple_of(chip * half_k, 128), half_k)
        return jnp.dot(joined, wo[k_rows, :], preferred_element_type=f32)

    for w in att_near:
        w()
    part_other[...] = project(1 - side, side)
    att_far = [r() for r in att_relay[:2]]
    part_self[...] = project(side, side)
    att_far += [r() for r in att_relay[2:hps]]
    for w in att_far:
        w()
    made = (part_other[...] + project(1 - side, 1 - side)).astype(bf16)
    for k in range(2):
        for b in range(2):
            row = b * own + k * half
            po[k, b * half : (b + 1) * half, :] = made[row : row + half]
    final = [
        send(po.at[core], pr.at[p], fresh(), {"tp": p2}),
        send(po.at[1 - core], pr.at[p], fresh(), {"tp": p3}),
    ]
    att_far = [r() for r in att_relay[hps:]]
    for w in att_far:
        w()
    made = (part_self[...] + project(side, 1 - side)).astype(bf16)
    for k in range(2):
        for b in range(2):
            row = b * own + k * half
            po[2 + k, b * half : (b + 1) * half, :] = made[row : row + half]
    close = send(po.at[2 + 1 - core], pr.at[p], fresh(), {"tp": p1})

    stores = []

    def mix(j, source):
        cols = pl.ds(pl.multiple_of(j * modw, 128), modw)
        gate = mod[j, 4:5, :]
        for r in range(0, own, STEP):
            outv[r : r + STEP, cols] = (
                lat[p, r : r + STEP, cols].astype(f32)
                + gate * source[r : r + STEP, :].astype(f32)
            ).astype(bf16)
        copy = pltpu.make_async_copy(
            outv.at[:, cols], out_hbm.at[:, cols], out_sem.at[len(stores)]
        )
        copy.start()
        stores.append(copy)

    mix(p, po.at[2 + core])
    close.wait_recv()
    mix(p1, pr.at[p1])
    final[0].wait_recv()
    mix(p2, pr.at[p2])
    final[1].wait_recv()
    mix(p3, pr.at[p3])

    for copy in sends:
        copy.wait_send()
    for part in range(2):
        for kind in range(3):
            swap(z, part, kind).wait_send()

        @pl.when(has_right)
        def _():
            Hop(z, z + 1, 0, part).wait_send()

        @pl.when(has_left)
        def _():
            Hop(z, z - 1, 1, part).wait_send()

        def drain(o, way, onward, more):
            for kind in range(3):
                swap(o, part, kind).wait_send()

            @pl.when(more)
            def _():
                Hop(o, onward, way, part).wait_send()

        for step in range(spn - 1):
            at_distance(step, drain)
    for copy in stores:
        copy.wait()


def fused_device(
    latents,
    conditions,
    context,
    w_shift,
    w_scale,
    w_gate,
    w_qdown,
    w_kvdown,
    w_rope,
    q_gain,
    latent_norm_gain,
    query_up_weight,
    key_up_weight,
    value_up_weight,
    context_bias,
    w_out,
):
    f32, bf16 = jnp.float32, jnp.bfloat16
    spn = lax.axis_size("sp")
    own, width = latents.shape
    ctxn = context.shape[0]
    tok = 4 * own
    seg = tok + ctxn
    heads = context_bias.shape[0]
    modw = w_shift.shape[1]
    kdim, qcols = w_qdown.shape
    kcols = w_kvdown.shape[1]
    cosine, sine = turn_tables(spn, own)
    hbm = pl.BlockSpec(memory_space=pltpu.HBM)
    V, DMA = pltpu.VMEM, pltpu.SemaphoreType.DMA
    scratch = [
        V(conditions.shape, f32),
        pltpu.SMEM(context_bias.shape, f32),
        V((1,) + q_gain.shape, f32),
        V((1,) + latent_norm_gain.shape, f32),
        V(w_rope.shape[::-1], bf16),
        V((16, conditions.shape[1]), f32),
        V((3,) + w_shift.shape, bf16),
        V((4, own, width), bf16),
        V((ctxn, width), bf16),
        V((seg, width), bf16),
        V((kdim, qcols), bf16),
        V((kdim, kcols + 128), bf16),
        V((spn, 8, modw), f32),
        V((4, 8, modw), f32),
        V((4, 2, 2 * own, qcols), bf16),
        V((spn, 4, seg, kcols), bf16),
        V((spn, seg // 4, 128), bf16),
        V((seg, 128), f32),
        V((seg, 4 * kcols), bf16),
        V((tok, 4 * qcols), bf16),
        V(query_up_weight.shape, bf16),
        V(key_up_weight.shape, bf16),
        V(value_up_weight.shape, bf16),
        V(w_out.shape, bf16),
        V((tok, 128), f32),
        V((tok, 128), f32),
        V((heads, tok, 128), bf16),
        V((heads, seg, 128), bf16),
        V((heads, seg, 128), bf16),
        V((heads, tok, 128), f32),
        V((heads, tok, 128), f32),
        V((4, heads // 2, 2, 2, own, 128), bf16),
        V((4, own, modw), bf16),
        V((4, own, modw), bf16),
        V((seg, 128), f32),
        V((seg, 128), f32),
        V((2 * own, modw), f32),
        V((2 * own, modw), f32),
        V((own, width), bf16),
        DMA((18,)),
        DMA((48,)),
        DMA((48,)),
        DMA((2, 2, 2, spn)),
        DMA((2, 2, spn)),
        DMA((3, 2, spn)),
        DMA((3, 2, spn)),
        DMA((4,)),
    ]
    return pl.pallas_call(
        block_kernel,
        out_shape=jax.ShapeDtypeStruct(latents.shape, bf16),
        in_specs=[hbm] * 18,
        out_specs=hbm,
        scratch_shapes=scratch,
        compiler_params=pltpu.CompilerParams(
            collective_id=0, has_side_effects=True, vmem_limit_bytes=56 * 1024 * 1024
        ),
    )(
        conditions,
        context_bias,
        q_gain[None, :],
        latent_norm_gain[None, :],
        w_rope.T,
        latents,
        context,
        w_shift,
        w_scale,
        w_gate,
        w_qdown,
        w_kvdown,
        query_up_weight,
        key_up_weight,
        value_up_weight,
        w_out,
        jnp.asarray(cosine),
        jnp.asarray(sine),
    )


def on_device(*arrays):
    latents, context, bias = arrays[0], arrays[2], arrays[14]
    fits = (
        lax.axis_size("tp") == 4
        and latents.shape[0] % 32 == 0
        and context.shape[0] % 128 == 0
        and latents.shape[0] > 2 * BAND
        and (4 * latents.shape[0] + context.shape[0]) == 512
        and arrays[6].shape[1] == 256
        and arrays[7].shape[1] == 128
        and bias.shape[0] == 8
    )
    return fused_device(*arrays) if fits else plain_device(*arrays)


def solution(mesh):
    in_specs = (
        P(("grp", "sp", "tp"), None),
        P("grp", "sp"),
        P(("grp", "sp"), None),
        P("sp", "tp"),
        P("sp", "tp"),
        P("sp", "tp"),
        P(None, "tp"),
        P(None, "tp"),
        P(),
        P(),
        P(),
        P(None, "tp"),
        P(None, "tp"),
        P(None, "tp"),
        P("tp"),
        P(None, "tp"),
    )
    out_specs = P(("grp", "sp", "tp"), None)
    return jax.shard_map(
        on_device, mesh=mesh, in_specs=in_specs, out_specs=out_specs, check_vma=False
    )
```

```python
import functools

import jax
import jax.numpy as jnp
import numpy as np
from jax import lax
from jax.experimental import pallas as pl
from jax.experimental.pallas import tpu as pltpu
from jax.sharding import PartitionSpec as P

PLAIN_QK_DIM = 64
ROTARY_DIM = 32
VALUE_DIM = 64
GRID_W = 64


EPSILON = 1e-06
NEGATIVE = -1e30


def layer_modulate(row_block, shift_by, scale_by):
    values = row_block.astype(jnp.float32)
    center = values - jnp.mean(values, axis=-1, keepdims=True)
    spread = jnp.mean(center * center, axis=-1, keepdims=True)
    normed = center * lax.rsqrt(spread + EPSILON)
    return (normed * (1.0 + scale_by) + shift_by).astype(jnp.bfloat16)


def rms_scale(raw_rows, gain_vec):
    values = raw_rows.astype(jnp.float32)
    factor = lax.rsqrt(jnp.mean(values * values, axis=-1, keepdims=True) + EPSILON)
    return (values * factor * gain_vec).astype(jnp.bfloat16)


def axial_turn(values, positions):
    freq_count = values.shape[-1] // 4
    inverse = 10000.0 ** (-jnp.arange(freq_count, dtype=jnp.float32) / freq_count)
    grid_row = (positions // GRID_W).astype(jnp.float32)
    grid_col = (positions % GRID_W).astype(jnp.float32)
    target = (positions.shape[0],) + (1,) * (values.ndim - 2) + (freq_count,)
    pieces = []
    for half_index, coordinate in enumerate((grid_row, grid_col)):
        angles = (coordinate[:, None] * inverse[None, :]).reshape(target)
        cosine = jnp.cos(angles)
        sine_of = jnp.sin(angles)
        segment = values[..., 2 * half_index * freq_count : 2 * (half_index + 1) * freq_count]
        low_half = segment[..., :freq_count]
        high_half = segment[..., freq_count:]
        pieces.append(low_half * cosine - high_half * sine_of)
        pieces.append(low_half * sine_of + high_half * cosine)
    return jnp.concatenate(pieces, axis=-1)


def plain_device(
    latents,
    conditions,
    context,
    w_shift,
    w_scale,
    w_gate,
    w_qdown,
    w_kvdown,
    w_rope,
    q_gain,
    latent_norm_gain,
    query_up_weight,
    key_up_weight,
    value_up_weight,
    context_bias,
    w_out,
):
    tp_count = lax.axis_size("tp")
    tp_index = lax.axis_index("tp")
    sp_index = lax.axis_index("sp")
    own_rows = latents.shape[0]
    tok_count = own_rows * tp_count
    ctx_share = context.shape[0] // tp_count
    cond_act = jax.nn.silu(conditions).astype(jnp.bfloat16)
    partial_mod = jnp.concatenate(
        [
            jnp.dot(cond_act, w_shift, preferred_element_type=jnp.float32),
            jnp.dot(cond_act, w_scale, preferred_element_type=jnp.float32),
            jnp.dot(cond_act[0:1], w_gate, preferred_element_type=jnp.float32),
        ],
        axis=0,
    )
    summed = lax.psum(partial_mod, "sp")
    modulation = lax.all_gather(summed, "tp", axis=1, tiled=True)
    ctx_own = lax.dynamic_slice_in_dim(context, tp_index * ctx_share, ctx_share, 0)
    h_lat = layer_modulate(latents, modulation[0], modulation[2])
    h_ctx = layer_modulate(ctx_own, modulation[1], modulation[3])
    h_own = jnp.concatenate([h_lat, h_ctx], axis=0)
    rope_raw = jnp.dot(h_own, w_rope, preferred_element_type=jnp.float32)
    own_pos = sp_index * tok_count + tp_index * own_rows + jnp.arange(own_rows, dtype=jnp.int32)
    kr_lat = axial_turn(rope_raw[:own_rows], own_pos).astype(jnp.bfloat16)
    kr_ctx = rope_raw[own_rows:].astype(jnp.bfloat16)
    arrived = lax.all_gather(h_own, "tp", axis=0, tiled=True)
    projected = jnp.concatenate(
        [
            jnp.dot(arrived, w_qdown, preferred_element_type=jnp.float32),
            jnp.dot(arrived, w_kvdown, preferred_element_type=jnp.float32),
        ],
        axis=1,
    ).astype(jnp.bfloat16)
    q_cols = w_qdown.shape[1]
    grouped = projected.reshape(tp_count, own_rows + ctx_share, projected.shape[1])
    cq_cols = grouped[:, :own_rows, :q_cols].reshape(tok_count, q_cols)
    kvl_cols = grouped[:, :own_rows, q_cols:].reshape(tok_count, w_kvdown.shape[1])
    kvc_cols = grouped[:, own_rows:, q_cols:].reshape(tp_count * ctx_share, w_kvdown.shape[1])
    cq_raw, kvl_raw, kvc_raw, krl_all, krc_all = (
        lax.all_gather(cq_cols, "tp", axis=1, tiled=True),
        lax.all_gather(kvl_cols, "tp", axis=1, tiled=True),
        lax.all_gather(kvc_cols, "tp", axis=1, tiled=True),
        lax.all_gather(kr_lat, "tp", axis=0, tiled=True),
        lax.all_gather(kr_ctx, "tp", axis=0, tiled=True),
    )
    cq_all = rms_scale(cq_raw, q_gain)
    ckv_all = jnp.concatenate(
        [rms_scale(kvl_raw, latent_norm_gain), rms_scale(kvc_raw, latent_norm_gain)], axis=0
    )
    kr_all = jnp.concatenate([krl_all, krc_all], axis=0)
    head_count = query_up_weight.shape[1] // (PLAIN_QK_DIM + ROTARY_DIM)
    q_all = jnp.dot(cq_all, query_up_weight, preferred_element_type=jnp.float32)
    q_all = q_all.reshape(tok_count, head_count, PLAIN_QK_DIM + ROTARY_DIM)
    query_pos = sp_index * tok_count + jnp.arange(tok_count, dtype=jnp.int32)
    queries = jnp.concatenate(
        [q_all[..., :PLAIN_QK_DIM], axial_turn(q_all[..., PLAIN_QK_DIM:], query_pos)], axis=-1
    ).astype(jnp.bfloat16)
    q_nope = queries[..., :PLAIN_QK_DIM]
    q_rope = queries[..., PLAIN_QK_DIM:]
    seg_rows = ckv_all.shape[0]
    is_ctx = (jnp.arange(seg_rows, dtype=jnp.int32) >= tok_count).astype(jnp.float32)
    bias_row = context_bias[None, :, None] * is_ctx[None, None, :]
    score_scale = (PLAIN_QK_DIM + ROTARY_DIM) ** (-0.5)

    def attend_block(running, key_block, value_block, rope_block):
        running_max, running_sum, numerator = running
        scores = jnp.einsum("ihd,jhd->ihj", q_nope, key_block, preferred_element_type=jnp.float32)
        scores = scores + jnp.einsum(
            "ihd,jd->ihj", q_rope, rope_block, preferred_element_type=jnp.float32
        )
        scores = scores * score_scale + bias_row
        new_max = jnp.maximum(running_max, jnp.max(scores, axis=-1))
        rescale = jnp.exp(running_max - new_max)
        exponent = jnp.exp(scores - new_max[..., None])
        running_sum = running_sum * rescale + jnp.sum(exponent, axis=-1)
        numerator = numerator * rescale[..., None] + jnp.einsum(
            "ihj,jhd->ihd",
            exponent.astype(jnp.bfloat16),
            value_block,
            preferred_element_type=jnp.float32,
        )
        return (new_max, running_sum, numerator)

    initial = (
        jnp.full((tok_count, head_count), NEGATIVE, jnp.float32),
        jnp.zeros((tok_count, head_count), jnp.float32),
        jnp.zeros((tok_count, head_count, VALUE_DIM), jnp.float32),
    )

    def expand_latent(key_group):
        latent_rows, rope_block = key_group
        key_block = jnp.dot(latent_rows, key_up_weight, preferred_element_type=jnp.float32).astype(
            jnp.bfloat16
        )
        value_block = jnp.dot(
            latent_rows, value_up_weight, preferred_element_type=jnp.float32
        ).astype(jnp.bfloat16)
        return (
            key_block.reshape(seg_rows, head_count, PLAIN_QK_DIM),
            value_block.reshape(seg_rows, head_count, VALUE_DIM),
            rope_block,
        )

    members = (
        lax.all_gather(ckv_all, "sp", axis=0, tiled=True),
        lax.all_gather(kr_all, "sp", axis=0, tiled=True),
    )
    block_count = members[0].shape[0] // seg_rows
    stacked = tuple(
        (member.reshape((block_count, seg_rows) + member.shape[1:]) for member in members)
    )

    def step_fn(state, key_group):
        key_block, value_block, rope_block = expand_latent(key_group)
        return (attend_block(state, key_block, value_block, rope_block), None)

    result, unused = lax.scan(step_fn, initial, stacked)
    running_max, running_sum, numerator = result
    attended = (
        (numerator / running_sum[..., None])
        .astype(jnp.bfloat16)
        .reshape(tok_count, head_count * VALUE_DIM)
    )
    proj_cols = jnp.dot(
        lax.all_gather(attended, "tp", axis=1, tiled=True),
        w_out,
        preferred_element_type=jnp.float32,
    )
    proj_rows = lax.all_to_all(
        proj_cols.astype(jnp.bfloat16), "tp", split_axis=0, concat_axis=1, tiled=True
    )
    mixed_rows = latents.astype(jnp.float32) + modulation[4] * proj_rows.astype(jnp.float32)
    return mixed_rows.astype(jnp.bfloat16)


MESH = pl.DeviceIdType.MESH
LOG2E = 1.4426950408889634
STEP = 16
BAND = 32
RELAY_AFTER = 2


def turn_tables(blocks, own):
    freq_count = ROTARY_DIM // 4
    inverse = 10000.0 ** (-np.arange(freq_count) / freq_count)
    tokens = blocks * 4 * own
    position = np.arange(tokens).reshape(blocks, 4, 2, own // 2).swapaxes(1, 2).reshape(-1)
    cosine = np.zeros((tokens, 128), np.float32)
    sine = np.zeros((tokens, 128), np.float32)
    cosine[:, :PLAIN_QK_DIM] = 1.0
    for half_index, coordinate in enumerate((position // GRID_W, position % GRID_W)):
        angles = coordinate[:, None] * inverse[None, :]
        low = PLAIN_QK_DIM + 2 * half_index * freq_count
        high = low + freq_count
        cosine[:, low : low + freq_count] = np.cos(angles)
        cosine[:, high : high + freq_count] = np.cos(angles)
        sine[:, low : low + freq_count] = -np.sin(angles)
        sine[:, high : high + freq_count] = np.sin(angles)
    return cosine, sine


def lanes_of(shape):
    return lax.broadcasted_iota(jnp.int32, shape, len(shape) - 1)


def turned(values, cosine, sine):
    lane = lanes_of(values.shape)
    swapped = jnp.where(
        (lane // 8) % 2 == 0, pltpu.roll(values, 120, 1), pltpu.roll(values, 8, 1)
    )
    return values * cosine + swapped * sine


def block_kernel(
    cond_hbm,
    bias_hbm,
    qgain_hbm,
    kvgain_hbm,
    rope_hbm,
    lat_hbm,
    ctx_hbm,
    wsh_hbm,
    wsc_hbm,
    wga_hbm,
    wqd_hbm,
    wkd_hbm,
    wqu_hbm,
    wku_hbm,
    wvu_hbm,
    wo_hbm,
    cos_hbm,
    sin_hbm,
    out_ref,
    cond_ref,
    bias_ref,
    qgain_ref,
    kvgain_ref,
    rope_ref,
    cond16,
    w3,
    lat,
    ctx,
    hid,
    wqd,
    wkvr,
    modp,
    mod,
    cq,
    kvx,
    krx,
    kraw,
    ckn,
    cqn,
    wqu,
    wku,
    wvu,
    wo,
    cosv,
    sinv,
    qh,
    kb,
    vb,
    acc,
    mx,
    att,
    po,
    pr,
    st_mean,
    st_rate,
    part_self,
    part_other,
    load_sem,
    send_sem,
    recv_sem,
    zsend,
    zrecv,
    ssend,
    srecv,
):
    f32, bf16 = jnp.float32, jnp.bfloat16
    spn = lax.axis_size("sp")
    p = lax.axis_index("tp")
    z = lax.axis_index("sp")
    core = lax.rem(p, 2)
    side = p // 2
    p1, p2, p3 = p ^ 1, p ^ 2, p ^ 3
    own = lat.shape[1]
    width = lat.shape[2]
    half = own // 2
    tok = own * 4
    pair = own * 2
    ctxn = ctx.shape[0]
    seg = tok + ctxn
    arows = ctxn + pair
    modw = w3.shape[2]
    heads = qh.shape[0]
    kcols = kvx.shape[3]
    spans = ((0, arows), (arows, pair))

    loads = []

    def load(src, dst):
        copy = pltpu.make_async_copy(src, dst, load_sem.at[len(loads)])
        loads.append(copy)
        copy.start()
        return copy

    l_lat = load(lat_hbm, lat.at[p])
    l_cond = load(cond_hbm, cond_ref)
    l_rope = load(rope_hbm, rope_ref)
    l_w3 = [load(ref, w3.at[i]) for i, ref in enumerate((wsh_hbm, wsc_hbm, wga_hbm))]
    l_ctx = load(ctx_hbm, ctx)
    l_kd = load(wkd_hbm, wkvr.at[:, pl.ds(0, kcols)])
    l_qd = load(wqd_hbm, wqd)
    table_rows = pl.ds(pl.multiple_of(z * tok, 8), tok)
    l_cos = load(cos_hbm.at[table_rows], cosv)
    l_sin = load(sin_hbm.at[table_rows], sinv)
    l_ku = load(wku_hbm, wku)
    l_vu = load(wvu_hbm, wvu)
    l_qu = load(wqu_hbm, wqu)
    l_wo = load(wo_hbm, wo)
    l_small = [
        load(bias_hbm, bias_ref),
        load(qgain_hbm, qgain_ref),
        load(kvgain_hbm, kvgain_ref),
    ]

    barrier = pltpu.get_barrier_semaphore()
    for peer in (p1, p2, p3):
        pl.semaphore_signal(barrier, inc=1, device_id={"tp": peer}, device_id_type=MESH)
    for d in range(1, spn):
        pl.semaphore_signal(
            barrier, inc=1, device_id={"sp": lax.rem(z + d, spn)}, device_id_type=MESH
        )

    sends = []

    def copy_to(src, dst, s_sem, r_sem, target):
        return pltpu.make_async_remote_copy(
            src_ref=src,
            dst_ref=dst,
            send_sem=s_sem,
            recv_sem=r_sem,
            device_id=target,
            device_id_type=MESH,
        )

    def send(src, dst, index, target):
        copy = copy_to(src, dst, send_sem.at[index], recv_sem.at[index], target)
        copy.start()
        sends.append(copy)
        return copy

    counter = [0]

    def fresh():
        counter[0] += 1
        return counter[0] - 1

    def near(view):
        return send(view(p), view(p), fresh(), {"tp": p1}).wait_recv

    def far(view, far_view=None):
        far_view = far_view or view
        i2, i3 = fresh(), fresh()
        first = send(view(p), view(p), i2, {"tp": p2})

        def relay():
            first.wait_recv()
            return send(far_view(p2), far_view(p2), i3, {"tp": p1}).wait_recv

        return relay

    l_cond.wait()
    cond16[...] = jnp.zeros_like(cond16)
    cond16[0:2, :] = cond_ref[...]
    conditions = cond16[...]
    act = (conditions / (1.0 + jnp.exp(-conditions))).astype(bf16)
    l_rope.wait()
    for c in range(0, width, 128):
        wkvr[c : c + 128, kcols:] = jnp.concatenate(
            [
                jnp.swapaxes(rope_ref[:, c : c + 128].astype(f32), 0, 1).astype(bf16),
                jnp.zeros((128, wkvr.shape[1] - kcols - ROTARY_DIM), bf16),
            ],
            axis=1,
        )

    pl.semaphore_wait(barrier, 3 + spn - 1)

    l_lat.wait()
    pieces_a = [(0, BAND), (BAND, half - BAND)]
    pieces_b = [(half, BAND), (half + BAND, half - BAND)]

    def piece_of(r, n):
        return lambda slot: lat.at[slot, pl.ds(r, n)]

    relay_lat = [far(piece_of(*piece)) for piece in pieces_a]
    lat_near = near(lambda slot: lat.at[slot])

    for i in range(3):
        l_w3[i].wait()
        partial_mod = jnp.dot(act, w3[i], preferred_element_type=f32)
        modp[z, 2 * i : 2 * i + 2, :] = partial_mod[0:2]
    modp[z, 6:8, :] = jnp.zeros((2, modw), f32)
    mod_waits = []
    for d in range(1, spn):
        mod_waits.append(
            send(modp.at[z], modp.at[z], fresh(), {"sp": lax.rem(z + d, spn)})
        )

    def measured(src, row_count, dst_row, step=BAND):
        @pl.loop(0, row_count // step)
        def _(i):
            rows = pl.ds(pl.multiple_of(i * step, STEP), step)
            to = pl.ds(pl.multiple_of(dst_row + i * step, STEP), step)
            tiles = [slice(c, c + 128) for c in range(0, width, 128)]
            sums = jnp.zeros((step, 128), f32)
            for c in tiles:
                sums = sums + src[rows, c].astype(f32)
            mean = jnp.broadcast_to(
                jnp.sum(sums, axis=-1, keepdims=True) * (1.0 / width), (step, 128)
            )
            squares = jnp.zeros((step, 128), f32)
            for c in tiles:
                center = src[rows, c].astype(f32) - mean
                squares = squares + center * center
            spread_of = jnp.sum(squares, axis=-1, keepdims=True) * (1.0 / width)
            st_mean[to, :] = mean
            st_rate[to, :] = jnp.broadcast_to(lax.rsqrt(spread_of + EPSILON), (step, 128))

    def modulate(src, row_count, dst_row, which, step=BAND):
        @pl.loop(0, row_count // step)
        def _(i):
            rows = pl.ds(pl.multiple_of(i * step, STEP), step)
            to = pl.ds(pl.multiple_of(dst_row + i * step, STEP), step)
            mean, rate = st_mean[to, :], st_rate[to, :]
            for c in range(0, width, 128):
                j, k = c // modw, c % modw
                shift_by = mod[j, which : which + 1, k : k + 128]
                scale_by = mod[j, 2 + which : 3 + which, k : k + 128]
                normed = (src[rows, c : c + 128].astype(f32) - mean) * rate
                hid[to, c : c + 128] = (normed * (1.0 + scale_by) + shift_by).astype(bf16)

    def hid_row(dev, r):
        return ctxn + (r // half) * pair + dev * half + r % half

    def band_view(dev, b):
        return lat.at[dev, pl.ds(b * half, half)]

    def take(dev, piece):
        r, n = piece
        measured(lat.at[dev, pl.ds(r, n)], n, hid_row(dev, r), n)
        modulate(lat.at[dev, pl.ds(r, n)], n, hid_row(dev, r), 0, n)

    for b in range(2):
        measured(band_view(p, b), half, hid_row(p, b * half), half)
    l_ctx.wait()
    measured(ctx, ctxn, 0)
    for copy in mod_waits:
        copy.wait_recv()
    total = modp[0]
    for i in range(1, spn):
        total = total + modp[i]
    mod[p] = total
    mod_relay = far(lambda slot: mod.at[slot])
    mod_near = near(lambda slot: mod.at[slot])
    for piece in pieces_b:
        relay_lat.append(far(piece_of(*piece)))
    lat_near()
    for b in range(2):
        measured(band_view(p1, b), half, hid_row(p1, b * half), half)
    lat_far = [relay_lat[0]()]
    mod_far = mod_relay()
    mod_near()
    mod_far()
    modulate(ctx, ctxn, 0, 1)
    for dev in (p, p1):
        modulate(band_view(dev, 0), half, hid_row(dev, 0), 0, half)
    take(p2, pieces_a[0])
    lat_far.append(relay_lat[1]())
    take(p2, pieces_a[1])
    for n, piece in enumerate(pieces_a):
        lat_far[n]()
        take(p3, piece)

    def kv_piece(o, slot, part):
        first, count = spans[part]
        return kvx.at[o, slot, pl.ds(first, count)]

    def kr_piece(o, part):
        first, count = spans[part]
        return krx.at[o, pl.ds(first // 4, count // 4)]

    class Hop:
        def __init__(self, origin, target, way, part):
            views = (kv_piece(origin, p, part), kr_piece(origin, part))
            self.copies = [
                copy_to(
                    view,
                    view,
                    zsend.at[way, part, kind, origin],
                    zrecv.at[part, kind, origin],
                    {"sp": target},
                )
                for kind, view in enumerate(views)
            ]

        def start(self):
            for copy in self.copies:
                copy.start()

        def wait_recv(self):
            for copy in self.copies:
                copy.wait_recv()

        def wait_send(self):
            for copy in self.copies:
                copy.wait_send()

    def swap(o, part, kind):
        view = kv_piece(o, p2 if kind == 2 else p, part)
        target = p2 if kind == 0 else p1
        return copy_to(
            view, view, ssend.at[kind, part, o], srecv.at[kind, part, o], {"tp": target}
        )

    has_right = z + 1 < spn
    has_left = z >= 1

    def spread(o, part):
        swap(o, part, 0).start()
        swap(o, part, 1).start()

    def relay(o, part):
        swap(o, part, 0).wait_recv()
        swap(o, part, 2).start()

    def gathered(o, part):
        swap(o, part, 1).wait_recv()
        swap(o, part, 2).wait_recv()

    def at_distance(step, fn):
        left, right = z - 1 - step, z + 1 + step

        @pl.when(left >= 0)
        def _():
            fn(left, 0, z + 1, has_right)

        @pl.when(right < spn)
        def _():
            fn(right, 1, z - 1, has_left)

    def forward(step, part):
        def one(o, way, onward, more):
            Hop(o, z, way, part).wait_recv()

            @pl.when(more)
            def _():
                Hop(o, onward, way, part).start()

        at_distance(step, one)

    def down_kv(part):
        first, count = spans[part]
        both = jnp.dot(hid[first : first + count, :], wkvr[...], preferred_element_type=f32)
        kvx[z, p, first : first + count, :] = both[:, :kcols].astype(bf16)
        kraw[first : first + count, :] = pltpu.roll(both[:, kcols:], 64, 1)
        low = max(first, ctxn)
        tabled = slice(low - ctxn, first + count - ctxn)
        kraw[low : first + count, :] = turned(
            kraw[low : first + count, :], cosv[tabled, :], sinv[tabled, :]
        )
        for t in range(first // 64, (first + count) // 64):
            packed = None
            for j in range(4):
                row = 64 * t + j * STEP
                moved = pltpu.roll(kraw[row : row + STEP, :], (32 * j + 64) % 128, 1)
                packed = moved if packed is None else packed + moved
            krx[z, STEP * t : STEP * t + STEP, :] = packed.astype(bf16)
        spread(z, part)

        @pl.when(has_right)
        def _():
            Hop(z, z + 1, 0, part).start()

        @pl.when(has_left)
        def _():
            Hop(z, z - 1, 1, part).start()

    def down_q(part):
        first, count = spans[part]
        rows = slice(max(first, ctxn), first + count)
        cq[p, part] = jnp.dot(hid[rows, :], wqd[...], preferred_element_type=f32).astype(bf16)
        view = lambda slot: cq.at[slot, part]
        return far(view), near(view)

    l_kd.wait()
    l_qd.wait()
    l_cos.wait()
    l_sin.wait()
    down_kv(0)
    cq_a = down_q(0)
    for dev in (p, p1):
        modulate(band_view(dev, 1), half, hid_row(dev, half), 0, half)
    for n, piece in enumerate(pieces_b):
        lat_far.append(relay_lat[2 + n]())
        take(p2, piece)
    forward(0, 0)
    for n, piece in enumerate(pieces_b):
        lat_far[2 + n]()
        take(p3, piece)
    cq_b = down_q(1)
    down_kv(1)

    def rms(pieces, gain_ref, store):
        values = [piece.astype(f32) for piece in pieces]
        total_of = None
        for v in values:
            s = jnp.sum(v * v, axis=-1, keepdims=True)
            total_of = s if total_of is None else total_of + s
        cols = values[0].shape[1]
        factor = lax.rsqrt(total_of / (cols * len(values)) + EPSILON)
        for j, v in enumerate(values):
            gain = gain_ref[0:1, j * cols : (j + 1) * cols]
            store(slice(j * cols, (j + 1) * cols), (v * factor * gain).astype(bf16))

    def expand_half(block, hf):
        hrow = seg // 2
        for base in range(hf * hrow, (hf + 1) * hrow, 64):
            def put(cols, value, base=base):
                ckn[base : base + 64, cols] = value

            rms([kvx[block, r, base : base + 64, :] for r in range(4)], kvgain_ref, put)
        lane_h = lanes_of((hrow, 128))
        ones = (lane_h == VALUE_DIM).astype(f32)
        lane_s = lanes_of((STEP, 128))
        on_rope = (lane_s >= PLAIN_QK_DIM) & (lane_s < PLAIN_QK_DIM + ROTARY_DIM)
        rows = slice(hf * hrow, (hf + 1) * hrow)
        latent_rows = ckn[rows, :]
        pieces = []
        for t in range(4 * hf, 4 * hf + 4):
            packed = krx[block, STEP * t : STEP * t + STEP, :].astype(f32)
            for j in range(4):
                moved = pltpu.roll(packed, (192 - 32 * j) % 128, 1)
                pieces.append(jnp.where(on_rope, moved, 0.0))
        rope_key = jnp.concatenate(pieces, axis=0)
        keys = jnp.dot(latent_rows, wku[...], preferred_element_type=f32)
        vals = jnp.dot(latent_rows, wvu[...], preferred_element_type=f32)
        for hp in range(heads // 2):
            cols = slice(128 * hp, 128 * hp + 128)
            k2, v2 = keys[:, cols], vals[:, cols]
            kb[2 * hp, rows, :] = jnp.where(lane_h < 64, k2, rope_key).astype(bf16)
            kb[2 * hp + 1, rows, :] = jnp.where(
                lane_h < 64, pltpu.roll(k2, 64, 1), rope_key
            ).astype(bf16)
            vb[2 * hp, rows, :] = jnp.where(lane_h < 64, v2, ones).astype(bf16)
            vb[2 * hp + 1, rows, :] = jnp.where(
                lane_h < 64, pltpu.roll(v2, 64, 1), ones
            ).astype(bf16)

    def block_at(step):
        below = jnp.minimum(z, spn - 1 - z)
        near_block = jnp.where(lax.rem(step, 2) == 1, z - (step + 1) // 2, z + step // 2)
        past = jnp.where(z < spn - 1 - z, step, spn - 1 - step)
        return jnp.where(step <= 2 * below, near_block, past)

    lane = lanes_of((pair, 128))

    def up_q(b):
        for base in range(0, pair, 64):
            def put(cols, value, base=base):
                cqn[base : base + 64, cols] = value

            rms([cq[r, b, base : base + 64, :] for r in range(4)], qgain_ref, put)
        q_all = jnp.dot(cqn[...], wqu[...], preferred_element_type=f32)
        rows = slice(b * pair, (b + 1) * pair)
        for h in range(heads):
            offset = h * (PLAIN_QK_DIM + ROTARY_DIM)
            tile, shift = offset // 128, offset % 128
            head = q_all[:, 128 * tile : 128 * tile + 128]
            if shift:
                head = pltpu.roll(head, 128 - shift, 1)
                if shift + PLAIN_QK_DIM + ROTARY_DIM > 128:
                    rest = q_all[:, 128 * tile + 128 : 128 * tile + 256]
                    head = jnp.where(
                        lane < 128 - shift, head, pltpu.roll(rest, 128 - shift, 1)
                    )
            qh[h, rows, :] = turned(head, cosv[rows, :], sinv[rows, :]).astype(bf16)

    for copy in l_small:
        copy.wait()
    l_qu.wait()
    l_ku.wait()
    l_vu.wait()
    acc[...] = jnp.zeros_like(acc)
    mx[...] = jnp.full(mx.shape, NEGATIVE, f32)
    factor = (PLAIN_QK_DIM + ROTARY_DIM) ** (-0.5) * LOG2E
    blocks = [None] + [block_at(jnp.int32(step)) for step in range(1, spn)]

    spread(blocks[1], 0)
    cq_waits = [cq_a[1], cq_a[0]()]
    relay(z, 0)
    for w in cq_waits:
        w()
    up_q(0)
    forward(1, 0)
    gathered(z, 0)
    expand_half(z, 0)
    cq_waits = [cq_b[1], cq_b[0]()]
    relay(z, 1)
    forward(0, 1)
    spread(blocks[1], 1)
    spread(blocks[2], 0)
    for w in cq_waits:
        w()
    up_q(1)
    gathered(z, 1)
    expand_half(z, 1)

    def score(h):
        return lax.dot_general(
            qh[h], kb[h], (((1,), (1,)), ((), ())), preferred_element_type=f32
        )

    def attend(h, scores):
        tiles = [scores[:, c : c + 128] * factor for c in range(0, seg, 128)]
        bias = bias_ref[h] * LOG2E
        tiles = [t + bias if n * 128 < ctxn else t for n, t in enumerate(tiles)]
        best = functools.reduce(jnp.maximum, tiles)
        old = mx[h]
        new = jnp.maximum(old, jnp.max(best, axis=-1, keepdims=True))
        mx[h] = new
        weights = jnp.concatenate([jnp.exp2(t - new).astype(bf16) for t in tiles], axis=1)
        acc[h] = acc[h] * jnp.exp2(old - new) + jnp.dot(
            weights, vb[h], preferred_element_type=f32
        )

    def attend_all(after):
        scores = score(0)
        for h in range(heads):
            following = score(h + 1) if h + 1 < heads else None
            attend(h, scores)
            after(h)
            scores = following

    @pl.loop(1, spn)
    def _(step):
        block = block_at(step)

        def meanwhile(h):
            if h != RELAY_AFTER:
                return

            @pl.when(step == 1)
            def _():
                forward(2, 0)
                forward(1, 1)
                spread(blocks[2], 1)
                spread(blocks[3], 0)

            for part in range(2):
                relay(block, part)

            @pl.when(step == 2)
            def _():
                forward(2, 1)
                spread(blocks[3], 1)

        attend_all(meanwhile)
        for part in range(2):
            gathered(block, part)
        for hf in range(2):
            expand_half(block, hf)

    att_relay, att_near = [], []
    lane64 = lanes_of((tok, 128)) < VALUE_DIM
    quarter = own

    def finish(h):
        if h % 2 == 0:
            return
        hp = h // 2
        low, high = acc[h - 1], acc[h]
        totals = jnp.where(
            lane64, low[:, VALUE_DIM : VALUE_DIM + 1], high[:, VALUE_DIM : VALUE_DIM + 1]
        )
        value = (jnp.where(lane64, low, pltpu.roll(high, 64, 1)) / totals).astype(bf16)
        for b in range(2):
            for s in range(2):
                row = (2 * b + s) * quarter
                att[p, hp, b, s] = value[row : row + quarter]
        att_relay.append(
            far(
                lambda slot: att.at[slot, hp, :, side],
                lambda slot: att.at[slot, hp, :, 1 - side],
            )
        )
        att_near.append(near(lambda slot: att.at[slot, hp]))

    attend_all(finish)

    hps = heads // 2
    for first in range(0, hps, 2):
        att_relay.append(
            far(
                lambda slot, first=first: att.at[slot, pl.ds(first, 2), :, 1 - side],
                lambda slot, first=first: att.at[slot, pl.ds(first, 2), :, side],
            )
        )
    l_wo.wait()
    half_k = heads * VALUE_DIM * 2

    def project(rows_side, chip):
        joined = jnp.concatenate(
            [
                jnp.concatenate([att[2 * chip + r, hp, b, rows_side] for b in range(2)], axis=0)
                for r in range(2)
                for hp in range(hps)
            ],
            axis=1,
        )
        k_rows = pl.ds(pl.multiple_of(chip * half_k, 128), half_k)
        return jnp.dot(joined, wo[k_rows, :], preferred_element_type=f32)

    for w in att_near:
        w()
    part_other[...] = project(1 - side, side)
    att_far = [r() for r in att_relay[:2]]
    part_self[...] = project(side, side)
    att_far += [r() for r in att_relay[2:hps]]
    for w in att_far:
        w()
    made = (part_other[...] + project(1 - side, 1 - side)).astype(bf16)
    for k in range(2):
        for b in range(2):
            row = b * own + k * half
            po[k, b * half : (b + 1) * half, :] = made[row : row + half]
    final = [
        send(po.at[core], pr.at[p], fresh(), {"tp": p2}),
        send(po.at[1 - core], pr.at[p], fresh(), {"tp": p3}),
    ]
    att_far = [r() for r in att_relay[hps:]]
    for w in att_far:
        w()
    made = (part_self[...] + project(side, 1 - side)).astype(bf16)
    for k in range(2):
        for b in range(2):
            row = b * own + k * half
            po[2 + k, b * half : (b + 1) * half, :] = made[row : row + half]
    close = send(po.at[2 + 1 - core], pr.at[p], fresh(), {"tp": p1})

    def mix(j, source):
        cols = pl.ds(pl.multiple_of(j * modw, 128), modw)
        gate = mod[j, 4:5, :]
        for r in range(0, own, STEP):
            out_ref[r : r + STEP, cols] = (
                lat[p, r : r + STEP, cols].astype(f32)
                + gate * source[r : r + STEP, :].astype(f32)
            ).astype(bf16)

    mix(p, po.at[2 + core])
    close.wait_recv()
    mix(p1, pr.at[p1])
    final[0].wait_recv()
    mix(p2, pr.at[p2])
    final[1].wait_recv()
    mix(p3, pr.at[p3])

    for copy in sends:
        copy.wait_send()
    for part in range(2):
        for kind in range(3):
            swap(z, part, kind).wait_send()

        @pl.when(has_right)
        def _():
            Hop(z, z + 1, 0, part).wait_send()

        @pl.when(has_left)
        def _():
            Hop(z, z - 1, 1, part).wait_send()

        def drain(o, way, onward, more):
            for kind in range(3):
                swap(o, part, kind).wait_send()

            @pl.when(more)
            def _():
                Hop(o, onward, way, part).wait_send()

        for step in range(spn - 1):
            at_distance(step, drain)


def fused_device(
    latents,
    conditions,
    context,
    w_shift,
    w_scale,
    w_gate,
    w_qdown,
    w_kvdown,
    w_rope,
    q_gain,
    latent_norm_gain,
    query_up_weight,
    key_up_weight,
    value_up_weight,
    context_bias,
    w_out,
):
    f32, bf16 = jnp.float32, jnp.bfloat16
    spn = lax.axis_size("sp")
    own, width = latents.shape
    ctxn = context.shape[0]
    tok = 4 * own
    seg = tok + ctxn
    heads = context_bias.shape[0]
    modw = w_shift.shape[1]
    kdim, qcols = w_qdown.shape
    kcols = w_kvdown.shape[1]
    cosine, sine = turn_tables(spn, own)
    hbm = pl.BlockSpec(memory_space=pltpu.HBM)
    V, DMA = pltpu.VMEM, pltpu.SemaphoreType.DMA
    scratch = [
        V(conditions.shape, f32),
        pltpu.SMEM(context_bias.shape, f32),
        V((1,) + q_gain.shape, f32),
        V((1,) + latent_norm_gain.shape, f32),
        V(w_rope.shape[::-1], bf16),
        V((16, conditions.shape[1]), f32),
        V((3,) + w_shift.shape, bf16),
        V((4, own, width), bf16),
        V((ctxn, width), bf16),
        V((seg, width), bf16),
        V((kdim, qcols), bf16),
        V((kdim, kcols + 128), bf16),
        V((spn, 8, modw), f32),
        V((4, 8, modw), f32),
        V((4, 2, 2 * own, qcols), bf16),
        V((spn, 4, seg, kcols), bf16),
        V((spn, seg // 4, 128), bf16),
        V((seg, 128), f32),
        V((seg, 4 * kcols), bf16),
        V((2 * own, 4 * qcols), bf16),
        V(query_up_weight.shape, bf16),
        V(key_up_weight.shape, bf16),
        V(value_up_weight.shape, bf16),
        V(w_out.shape, bf16),
        V((tok, 128), f32),
        V((tok, 128), f32),
        V((heads, tok, 128), bf16),
        V((heads, seg, 128), bf16),
        V((heads, seg, 128), bf16),
        V((heads, tok, 128), f32),
        V((heads, tok, 128), f32),
        V((4, heads // 2, 2, 2, own, 128), bf16),
        V((4, own, modw), bf16),
        V((4, own, modw), bf16),
        V((seg, 128), f32),
        V((seg, 128), f32),
        V((2 * own, modw), f32),
        V((2 * own, modw), f32),
        DMA((18,)),
        DMA((48,)),
        DMA((48,)),
        DMA((2, 2, 2, spn)),
        DMA((2, 2, spn)),
        DMA((3, 2, spn)),
        DMA((3, 2, spn)),
    ]
    return pl.pallas_call(
        block_kernel,
        out_shape=pltpu.VMEM(latents.shape, bf16),
        in_specs=[hbm] * 18,
        out_specs=pl.BlockSpec(memory_space=pltpu.VMEM),
        scratch_shapes=scratch,
        compiler_params=pltpu.CompilerParams(
            collective_id=0, has_side_effects=True, vmem_limit_bytes=56 * 1024 * 1024
        ),
    )(
        conditions,
        context_bias,
        q_gain[None, :],
        latent_norm_gain[None, :],
        w_rope.T,
        latents,
        context,
        w_shift,
        w_scale,
        w_gate,
        w_qdown,
        w_kvdown,
        query_up_weight,
        key_up_weight,
        value_up_weight,
        w_out,
        jnp.asarray(cosine),
        jnp.asarray(sine),
    )


def on_device(*arrays):
    latents, context, bias = arrays[0], arrays[2], arrays[14]
    fits = (
        lax.axis_size("tp") == 4
        and lax.axis_size("sp") == 4
        and latents.shape[0] % 32 == 0
        and context.shape[0] % 128 == 0
        and latents.shape[0] > 2 * BAND
        and (4 * latents.shape[0] + context.shape[0]) == 512
        and arrays[6].shape[1] == 256
        and arrays[7].shape[1] == 128
        and bias.shape[0] == 8
    )
    return fused_device(*arrays) if fits else plain_device(*arrays)


def solution(mesh):
    in_specs = (
        P(("grp", "sp", "tp"), None),
        P("grp", "sp"),
        P(("grp", "sp"), None),
        P("sp", "tp"),
        P("sp", "tp"),
        P("sp", "tp"),
        P(None, "tp"),
        P(None, "tp"),
        P(),
        P(),
        P(),
        P(None, "tp"),
        P(None, "tp"),
        P(None, "tp"),
        P("tp"),
        P(None, "tp"),
    )
    out_specs = P(("grp", "sp", "tp"), None)
    return jax.shard_map(
        on_device, mesh=mesh, in_specs=in_specs, out_specs=out_specs, check_vma=False
    )
```

```python
import functools

import jax
import jax.numpy as jnp
import numpy as np
from jax import lax
from jax.experimental import pallas as pl
from jax.experimental.pallas import tpu as pltpu
from jax.sharding import PartitionSpec as P

PLAIN_QK_DIM = 64
ROTARY_DIM = 32
VALUE_DIM = 64
GRID_W = 64


EPSILON = 1e-06
NEGATIVE = -1e30


def layer_modulate(row_block, shift_by, scale_by):
    values = row_block.astype(jnp.float32)
    center = values - jnp.mean(values, axis=-1, keepdims=True)
    spread = jnp.mean(center * center, axis=-1, keepdims=True)
    normed = center * lax.rsqrt(spread + EPSILON)
    return (normed * (1.0 + scale_by) + shift_by).astype(jnp.bfloat16)


def rms_scale(raw_rows, gain_vec):
    values = raw_rows.astype(jnp.float32)
    factor = lax.rsqrt(jnp.mean(values * values, axis=-1, keepdims=True) + EPSILON)
    return (values * factor * gain_vec).astype(jnp.bfloat16)


def axial_turn(values, positions):
    freq_count = values.shape[-1] // 4
    inverse = 10000.0 ** (-jnp.arange(freq_count, dtype=jnp.float32) / freq_count)
    grid_row = (positions // GRID_W).astype(jnp.float32)
    grid_col = (positions % GRID_W).astype(jnp.float32)
    target = (positions.shape[0],) + (1,) * (values.ndim - 2) + (freq_count,)
    pieces = []
    for half_index, coordinate in enumerate((grid_row, grid_col)):
        angles = (coordinate[:, None] * inverse[None, :]).reshape(target)
        cosine = jnp.cos(angles)
        sine_of = jnp.sin(angles)
        segment = values[..., 2 * half_index * freq_count : 2 * (half_index + 1) * freq_count]
        low_half = segment[..., :freq_count]
        high_half = segment[..., freq_count:]
        pieces.append(low_half * cosine - high_half * sine_of)
        pieces.append(low_half * sine_of + high_half * cosine)
    return jnp.concatenate(pieces, axis=-1)


def plain_device(
    latents,
    conditions,
    context,
    w_shift,
    w_scale,
    w_gate,
    w_qdown,
    w_kvdown,
    w_rope,
    q_gain,
    latent_norm_gain,
    query_up_weight,
    key_up_weight,
    value_up_weight,
    context_bias,
    w_out,
):
    tp_count = lax.axis_size("tp")
    tp_index = lax.axis_index("tp")
    sp_index = lax.axis_index("sp")
    own_rows = latents.shape[0]
    tok_count = own_rows * tp_count
    ctx_share = context.shape[0] // tp_count
    cond_act = jax.nn.silu(conditions).astype(jnp.bfloat16)
    partial_mod = jnp.concatenate(
        [
            jnp.dot(cond_act, w_shift, preferred_element_type=jnp.float32),
            jnp.dot(cond_act, w_scale, preferred_element_type=jnp.float32),
            jnp.dot(cond_act[0:1], w_gate, preferred_element_type=jnp.float32),
        ],
        axis=0,
    )
    summed = lax.psum(partial_mod, "sp")
    modulation = lax.all_gather(summed, "tp", axis=1, tiled=True)
    ctx_own = lax.dynamic_slice_in_dim(context, tp_index * ctx_share, ctx_share, 0)
    h_lat = layer_modulate(latents, modulation[0], modulation[2])
    h_ctx = layer_modulate(ctx_own, modulation[1], modulation[3])
    h_own = jnp.concatenate([h_lat, h_ctx], axis=0)
    rope_raw = jnp.dot(h_own, w_rope, preferred_element_type=jnp.float32)
    own_pos = sp_index * tok_count + tp_index * own_rows + jnp.arange(own_rows, dtype=jnp.int32)
    kr_lat = axial_turn(rope_raw[:own_rows], own_pos).astype(jnp.bfloat16)
    kr_ctx = rope_raw[own_rows:].astype(jnp.bfloat16)
    arrived = lax.all_gather(h_own, "tp", axis=0, tiled=True)
    projected = jnp.concatenate(
        [
            jnp.dot(arrived, w_qdown, preferred_element_type=jnp.float32),
            jnp.dot(arrived, w_kvdown, preferred_element_type=jnp.float32),
        ],
        axis=1,
    ).astype(jnp.bfloat16)
    q_cols = w_qdown.shape[1]
    grouped = projected.reshape(tp_count, own_rows + ctx_share, projected.shape[1])
    cq_cols = grouped[:, :own_rows, :q_cols].reshape(tok_count, q_cols)
    kvl_cols = grouped[:, :own_rows, q_cols:].reshape(tok_count, w_kvdown.shape[1])
    kvc_cols = grouped[:, own_rows:, q_cols:].reshape(tp_count * ctx_share, w_kvdown.shape[1])
    cq_raw, kvl_raw, kvc_raw, krl_all, krc_all = (
        lax.all_gather(cq_cols, "tp", axis=1, tiled=True),
        lax.all_gather(kvl_cols, "tp", axis=1, tiled=True),
        lax.all_gather(kvc_cols, "tp", axis=1, tiled=True),
        lax.all_gather(kr_lat, "tp", axis=0, tiled=True),
        lax.all_gather(kr_ctx, "tp", axis=0, tiled=True),
    )
    cq_all = rms_scale(cq_raw, q_gain)
    ckv_all = jnp.concatenate(
        [rms_scale(kvl_raw, latent_norm_gain), rms_scale(kvc_raw, latent_norm_gain)], axis=0
    )
    kr_all = jnp.concatenate([krl_all, krc_all], axis=0)
    head_count = query_up_weight.shape[1] // (PLAIN_QK_DIM + ROTARY_DIM)
    q_all = jnp.dot(cq_all, query_up_weight, preferred_element_type=jnp.float32)
    q_all = q_all.reshape(tok_count, head_count, PLAIN_QK_DIM + ROTARY_DIM)
    query_pos = sp_index * tok_count + jnp.arange(tok_count, dtype=jnp.int32)
    queries = jnp.concatenate(
        [q_all[..., :PLAIN_QK_DIM], axial_turn(q_all[..., PLAIN_QK_DIM:], query_pos)], axis=-1
    ).astype(jnp.bfloat16)
    q_nope = queries[..., :PLAIN_QK_DIM]
    q_rope = queries[..., PLAIN_QK_DIM:]
    seg_rows = ckv_all.shape[0]
    is_ctx = (jnp.arange(seg_rows, dtype=jnp.int32) >= tok_count).astype(jnp.float32)
    bias_row = context_bias[None, :, None] * is_ctx[None, None, :]
    score_scale = (PLAIN_QK_DIM + ROTARY_DIM) ** (-0.5)

    def attend_block(running, key_block, value_block, rope_block):
        running_max, running_sum, numerator = running
        scores = jnp.einsum("ihd,jhd->ihj", q_nope, key_block, preferred_element_type=jnp.float32)
        scores = scores + jnp.einsum(
            "ihd,jd->ihj", q_rope, rope_block, preferred_element_type=jnp.float32
        )
        scores = scores * score_scale + bias_row
        new_max = jnp.maximum(running_max, jnp.max(scores, axis=-1))
        rescale = jnp.exp(running_max - new_max)
        exponent = jnp.exp(scores - new_max[..., None])
        running_sum = running_sum * rescale + jnp.sum(exponent, axis=-1)
        numerator = numerator * rescale[..., None] + jnp.einsum(
            "ihj,jhd->ihd",
            exponent.astype(jnp.bfloat16),
            value_block,
            preferred_element_type=jnp.float32,
        )
        return (new_max, running_sum, numerator)

    initial = (
        jnp.full((tok_count, head_count), NEGATIVE, jnp.float32),
        jnp.zeros((tok_count, head_count), jnp.float32),
        jnp.zeros((tok_count, head_count, VALUE_DIM), jnp.float32),
    )

    def expand_latent(key_group):
        latent_rows, rope_block = key_group
        key_block = jnp.dot(latent_rows, key_up_weight, preferred_element_type=jnp.float32).astype(
            jnp.bfloat16
        )
        value_block = jnp.dot(
            latent_rows, value_up_weight, preferred_element_type=jnp.float32
        ).astype(jnp.bfloat16)
        return (
            key_block.reshape(seg_rows, head_count, PLAIN_QK_DIM),
            value_block.reshape(seg_rows, head_count, VALUE_DIM),
            rope_block,
        )

    members = (
        lax.all_gather(ckv_all, "sp", axis=0, tiled=True),
        lax.all_gather(kr_all, "sp", axis=0, tiled=True),
    )
    block_count = members[0].shape[0] // seg_rows
    stacked = tuple(
        (member.reshape((block_count, seg_rows) + member.shape[1:]) for member in members)
    )

    def step_fn(state, key_group):
        key_block, value_block, rope_block = expand_latent(key_group)
        return (attend_block(state, key_block, value_block, rope_block), None)

    result, unused = lax.scan(step_fn, initial, stacked)
    running_max, running_sum, numerator = result
    attended = (
        (numerator / running_sum[..., None])
        .astype(jnp.bfloat16)
        .reshape(tok_count, head_count * VALUE_DIM)
    )
    proj_cols = jnp.dot(
        lax.all_gather(attended, "tp", axis=1, tiled=True),
        w_out,
        preferred_element_type=jnp.float32,
    )
    proj_rows = lax.all_to_all(
        proj_cols.astype(jnp.bfloat16), "tp", split_axis=0, concat_axis=1, tiled=True
    )
    mixed_rows = latents.astype(jnp.float32) + modulation[4] * proj_rows.astype(jnp.float32)
    return mixed_rows.astype(jnp.bfloat16)


MESH = pl.DeviceIdType.MESH
LOG2E = 1.4426950408889634
STEP = 16
BAND = 32
RELAY_AFTER = 2


def turn_tables(blocks, own):
    freq_count = ROTARY_DIM // 4
    inverse = 10000.0 ** (-np.arange(freq_count) / freq_count)
    tokens = blocks * 4 * own
    position = np.arange(tokens).reshape(blocks, 4, 2, own // 2).swapaxes(1, 2).reshape(-1)
    cosine = np.zeros((tokens, 128), np.float32)
    sine = np.zeros((tokens, 128), np.float32)
    cosine[:, :PLAIN_QK_DIM] = 1.0
    for half_index, coordinate in enumerate((position // GRID_W, position % GRID_W)):
        angles = coordinate[:, None] * inverse[None, :]
        low = PLAIN_QK_DIM + 2 * half_index * freq_count
        high = low + freq_count
        cosine[:, low : low + freq_count] = np.cos(angles)
        cosine[:, high : high + freq_count] = np.cos(angles)
        sine[:, low : low + freq_count] = -np.sin(angles)
        sine[:, high : high + freq_count] = np.sin(angles)
    return cosine, sine


def lanes_of(shape):
    return lax.broadcasted_iota(jnp.int32, shape, len(shape) - 1)


def turned(values, cosine, sine):
    lane = lanes_of(values.shape)
    swapped = jnp.where(
        (lane // 8) % 2 == 0, pltpu.roll(values, 120, 1), pltpu.roll(values, 8, 1)
    )
    return values * cosine + swapped * sine


def block_kernel(
    cond_hbm,
    bias_hbm,
    qgain_hbm,
    kvgain_hbm,
    rope_hbm,
    lat_hbm,
    ctx_hbm,
    wsh_hbm,
    wsc_hbm,
    wga_hbm,
    wqd_hbm,
    wkd_hbm,
    wqu_hbm,
    wku_hbm,
    wvu_hbm,
    wo_hbm,
    cos_hbm,
    sin_hbm,
    out_ref,
    cond_ref,
    bias_ref,
    qgain_ref,
    kvgain_ref,
    rope_ref,
    cond16,
    w3,
    lat,
    ctx,
    hid,
    wqd,
    wkvr,
    modp,
    mod,
    cq,
    kvx,
    krx,
    kraw,
    ckn,
    cqn,
    wqu,
    wku,
    wvu,
    wo,
    cosv,
    sinv,
    qh,
    kb,
    vb,
    acc,
    mx,
    att,
    po,
    pr,
    st_mean,
    st_rate,
    part_self,
    part_other,
    load_sem,
    send_sem,
    recv_sem,
    zsend,
    zrecv,
    ssend,
    srecv,
):
    f32, bf16 = jnp.float32, jnp.bfloat16
    spn = lax.axis_size("sp")
    p = lax.axis_index("tp")
    z = lax.axis_index("sp")
    core = lax.rem(p, 2)
    side = p // 2
    p1, p2, p3 = p ^ 1, p ^ 2, p ^ 3
    own = lat.shape[1]
    width = lat.shape[2]
    half = own // 2
    tok = own * 4
    pair = own * 2
    ctxn = ctx.shape[0]
    seg = tok + ctxn
    arows = ctxn + pair
    modw = w3.shape[2]
    heads = qh.shape[0]
    kcols = kvx.shape[3]
    spans = ((0, arows), (arows, pair))

    loads = []

    def load(src, dst):
        copy = pltpu.make_async_copy(src, dst, load_sem.at[len(loads)])
        loads.append(copy)
        copy.start()
        return copy

    l_lat = load(lat_hbm, lat.at[p])
    l_cond = load(cond_hbm, cond_ref)
    l_rope = load(rope_hbm, rope_ref)
    l_w3 = [load(ref, w3.at[i]) for i, ref in enumerate((wsh_hbm, wsc_hbm, wga_hbm))]
    l_ctx = load(ctx_hbm, ctx)
    l_kd = load(wkd_hbm, wkvr.at[:, pl.ds(0, kcols)])
    l_qd = load(wqd_hbm, wqd)
    table_rows = pl.ds(pl.multiple_of(z * tok, 8), tok)
    l_cos = load(cos_hbm.at[table_rows], cosv)
    l_sin = load(sin_hbm.at[table_rows], sinv)
    l_ku = load(wku_hbm, wku)
    l_vu = load(wvu_hbm, wvu)
    l_qu = load(wqu_hbm, wqu)
    l_wo = load(wo_hbm, wo)
    l_small = [
        load(bias_hbm, bias_ref),
        load(qgain_hbm, qgain_ref),
        load(kvgain_hbm, kvgain_ref),
    ]

    barrier = pltpu.get_barrier_semaphore()
    for peer in (p1, p2, p3):
        pl.semaphore_signal(barrier, inc=1, device_id={"tp": peer}, device_id_type=MESH)
    for d in range(1, spn):
        pl.semaphore_signal(
            barrier, inc=1, device_id={"sp": lax.rem(z + d, spn)}, device_id_type=MESH
        )

    sends = []

    def copy_to(src, dst, s_sem, r_sem, target):
        return pltpu.make_async_remote_copy(
            src_ref=src,
            dst_ref=dst,
            send_sem=s_sem,
            recv_sem=r_sem,
            device_id=target,
            device_id_type=MESH,
        )

    def send(src, dst, index, target):
        copy = copy_to(src, dst, send_sem.at[index], recv_sem.at[index], target)
        copy.start()
        sends.append(copy)
        return copy

    counter = [0]

    def fresh():
        counter[0] += 1
        return counter[0] - 1

    def near(view):
        return send(view(p), view(p), fresh(), {"tp": p1}).wait_recv

    def far(view, far_view=None):
        far_view = far_view or view
        i2, i3 = fresh(), fresh()
        first = send(view(p), view(p), i2, {"tp": p2})

        def relay():
            first.wait_recv()
            return send(far_view(p2), far_view(p2), i3, {"tp": p1}).wait_recv

        return relay

    l_cond.wait()
    cond16[...] = jnp.zeros_like(cond16)
    cond16[0:2, :] = cond_ref[...]
    conditions = cond16[...]
    act = (conditions / (1.0 + jnp.exp(-conditions))).astype(bf16)
    l_rope.wait()
    for c in range(0, width, 128):
        wkvr[c : c + 128, kcols:] = jnp.concatenate(
            [
                jnp.swapaxes(rope_ref[:, c : c + 128].astype(f32), 0, 1).astype(bf16),
                jnp.zeros((128, wkvr.shape[1] - kcols - ROTARY_DIM), bf16),
            ],
            axis=1,
        )

    pl.semaphore_wait(barrier, 3 + spn - 1)

    l_lat.wait()
    pieces_a = [(0, BAND), (BAND, half - BAND)]
    pieces_b = [(half, BAND), (half + BAND, half - BAND)]

    def piece_of(r, n):
        return lambda slot: lat.at[slot, pl.ds(r, n)]

    relay_lat = [far(piece_of(*piece)) for piece in pieces_a]
    lat_near = near(lambda slot: lat.at[slot])

    for i in range(3):
        l_w3[i].wait()
        partial_mod = jnp.dot(act, w3[i], preferred_element_type=f32)
        modp[z, 2 * i : 2 * i + 2, :] = partial_mod[0:2]
    modp[z, 6:8, :] = jnp.zeros((2, modw), f32)
    mod_waits = []
    for d in range(1, spn):
        mod_waits.append(
            send(modp.at[z], modp.at[z], fresh(), {"sp": lax.rem(z + d, spn)})
        )

    def measured(src, row_count, dst_row, step=BAND):
        @pl.loop(0, row_count // step)
        def _(i):
            rows = pl.ds(pl.multiple_of(i * step, STEP), step)
            to = pl.ds(pl.multiple_of(dst_row + i * step, STEP), step)
            tiles = [slice(c, c + 128) for c in range(0, width, 128)]
            sums = jnp.zeros((step, 128), f32)
            for c in tiles:
                sums = sums + src[rows, c].astype(f32)
            mean = jnp.broadcast_to(
                jnp.sum(sums, axis=-1, keepdims=True) * (1.0 / width), (step, 128)
            )
            squares = jnp.zeros((step, 128), f32)
            for c in tiles:
                center = src[rows, c].astype(f32) - mean
                squares = squares + center * center
            spread_of = jnp.sum(squares, axis=-1, keepdims=True) * (1.0 / width)
            st_mean[to, :] = mean
            st_rate[to, :] = jnp.broadcast_to(lax.rsqrt(spread_of + EPSILON), (step, 128))

    def modulate(src, row_count, dst_row, which, step=BAND):
        @pl.loop(0, row_count // step)
        def _(i):
            rows = pl.ds(pl.multiple_of(i * step, STEP), step)
            to = pl.ds(pl.multiple_of(dst_row + i * step, STEP), step)
            mean, rate = st_mean[to, :], st_rate[to, :]
            for c in range(0, width, 128):
                j, k = c // modw, c % modw
                shift_by = mod[j, which : which + 1, k : k + 128]
                scale_by = mod[j, 2 + which : 3 + which, k : k + 128]
                normed = (src[rows, c : c + 128].astype(f32) - mean) * rate
                hid[to, c : c + 128] = (normed * (1.0 + scale_by) + shift_by).astype(bf16)

    def hid_row(dev, r):
        return ctxn + (r // half) * pair + dev * half + r % half

    def band_view(dev, b):
        return lat.at[dev, pl.ds(b * half, half)]

    def take(dev, piece):
        r, n = piece
        measured(lat.at[dev, pl.ds(r, n)], n, hid_row(dev, r), n)
        modulate(lat.at[dev, pl.ds(r, n)], n, hid_row(dev, r), 0, n)

    for b in range(2):
        measured(band_view(p, b), half, hid_row(p, b * half), half)
    l_ctx.wait()
    measured(ctx, ctxn, 0)
    for copy in mod_waits:
        copy.wait_recv()
    total = modp[0]
    for i in range(1, spn):
        total = total + modp[i]
    mod[p] = total
    mod_relay = far(lambda slot: mod.at[slot])
    mod_near = near(lambda slot: mod.at[slot])
    for piece in pieces_b:
        relay_lat.append(far(piece_of(*piece)))
    lat_near()
    for b in range(2):
        measured(band_view(p1, b), half, hid_row(p1, b * half), half)
    lat_far = [relay_lat[0]()]
    mod_far = mod_relay()
    mod_near()
    mod_far()
    modulate(ctx, ctxn, 0, 1)
    for dev in (p, p1):
        modulate(band_view(dev, 0), half, hid_row(dev, 0), 0, half)
    take(p2, pieces_a[0])
    lat_far.append(relay_lat[1]())
    take(p2, pieces_a[1])
    for n, piece in enumerate(pieces_a):
        lat_far[n]()
        take(p3, piece)

    def kv_piece(o, slot, part):
        first, count = spans[part]
        return kvx.at[o, slot, pl.ds(first, count)]

    def kr_piece(o, part):
        first, count = spans[part]
        return krx.at[o, pl.ds(first // 4, count // 4)]

    class Hop:
        def __init__(self, origin, target, way, part, lane_of=None):
            lane_of = origin if lane_of is None else lane_of
            views = (kv_piece(origin, p, part), kr_piece(origin, part))
            self.copies = [
                copy_to(
                    view,
                    view,
                    zsend.at[way, part, kind, lane_of],
                    zrecv.at[part, kind, origin],
                    {"sp": target},
                )
                for kind, view in enumerate(views)
            ]

        def start(self):
            for copy in self.copies:
                copy.start()

        def wait_recv(self):
            for copy in self.copies:
                copy.wait_recv()

        def wait_send(self):
            for copy in self.copies:
                copy.wait_send()

    def swap(o, part, kind):
        view = kv_piece(o, p2 if kind == 2 else p, part)
        target = p2 if kind == 0 else p1
        return copy_to(
            view, view, ssend.at[kind, part, o], srecv.at[kind, part, o], {"tp": target}
        )

    has_right = z + 1 < spn
    has_left = z >= 1

    def spread(o, part):
        swap(o, part, 0).start()
        swap(o, part, 1).start()

    def relay(o, part):
        swap(o, part, 0).wait_recv()
        swap(o, part, 2).start()

    def gathered(o, part):
        swap(o, part, 1).wait_recv()
        swap(o, part, 2).wait_recv()

    def at_distance(step, fn):
        left, right = z - 1 - step, z + 1 + step

        @pl.when(left >= 0)
        def _():
            fn(left, 0, z + 1, has_right)

        @pl.when(right < spn)
        def _():
            fn(right, 1, z - 1, has_left)

    def passed_on(step):
        return step + 2 < spn - 1

    def at_far_end(fn):
        at_distance(spn - 2, lambda target, way, onward, more: fn(target, 1 - way))

    def forward(step, part):
        def one(o, way, onward, more):
            Hop(o, z, way, part).wait_recv()
            if passed_on(step):

                @pl.when(more)
                def _():
                    Hop(o, onward, way, part).start()

        at_distance(step, one)

    def at_distances(fn):
        for step in range(spn - 1):
            at_distance(step, lambda target, way, onward, more: fn(target, 1 - way))

    def arrive(o):
        Hop(o, z, 0, 1).wait_recv()
        spread(o, 1)

    def down_kv(part):
        first, count = spans[part]
        both = jnp.dot(hid[first : first + count, :], wkvr[...], preferred_element_type=f32)
        kvx[z, p, first : first + count, :] = both[:, :kcols].astype(bf16)
        kraw[first : first + count, :] = pltpu.roll(both[:, kcols:], 64, 1)
        low = max(first, ctxn)
        tabled = slice(low - ctxn, first + count - ctxn)
        kraw[low : first + count, :] = turned(
            kraw[low : first + count, :], cosv[tabled, :], sinv[tabled, :]
        )
        for t in range(first // 64, (first + count) // 64):
            packed = None
            for j in range(4):
                row = 64 * t + j * STEP
                moved = pltpu.roll(kraw[row : row + STEP, :], (32 * j + 64) % 128, 1)
                packed = moved if packed is None else packed + moved
            krx[z, STEP * t : STEP * t + STEP, :] = packed.astype(bf16)
        spread(z, part)

        if part == 0:

            @pl.when(has_right)
            def _():
                Hop(z, z + 1, 0, part).start()

            @pl.when(has_left)
            def _():
                Hop(z, z - 1, 1, part).start()

            at_far_end(lambda target, way: Hop(z, target, way, part, target).start())
        else:
            at_distances(lambda target, way: Hop(z, target, way, part, target).start())

    def down_q(part):
        first, count = spans[part]
        rows = slice(max(first, ctxn), first + count)
        cq[p, part] = jnp.dot(hid[rows, :], wqd[...], preferred_element_type=f32).astype(bf16)
        view = lambda slot: cq.at[slot, part]
        return far(view), near(view)

    l_kd.wait()
    l_qd.wait()
    l_cos.wait()
    l_sin.wait()
    down_kv(0)
    cq_a = down_q(0)
    for dev in (p, p1):
        modulate(band_view(dev, 1), half, hid_row(dev, half), 0, half)
    for n, piece in enumerate(pieces_b):
        lat_far.append(relay_lat[2 + n]())
        take(p2, piece)
    forward(0, 0)
    for n, piece in enumerate(pieces_b):
        lat_far[2 + n]()
        take(p3, piece)
    cq_b = down_q(1)
    down_kv(1)

    def rms(pieces, gain_ref, store):
        values = [piece.astype(f32) for piece in pieces]
        total_of = None
        for v in values:
            s = jnp.sum(v * v, axis=-1, keepdims=True)
            total_of = s if total_of is None else total_of + s
        cols = values[0].shape[1]
        factor = lax.rsqrt(total_of / (cols * len(values)) + EPSILON)
        for j, v in enumerate(values):
            gain = gain_ref[0:1, j * cols : (j + 1) * cols]
            store(slice(j * cols, (j + 1) * cols), (v * factor * gain).astype(bf16))

    def expand_half(block, hf, slot=0):
        hrow = seg // 2
        for base in range(hf * hrow, (hf + 1) * hrow, 64):
            def put(cols, value, base=base):
                ckn[base : base + 64, cols] = value

            rms([kvx[block, r, base : base + 64, :] for r in range(4)], kvgain_ref, put)
        lane_h = lanes_of((hrow, 128))
        ones = (lane_h == VALUE_DIM).astype(f32)
        ones_odd = (lane_h == 0).astype(f32)
        lane_s = lanes_of((STEP, 128))
        on_rope = (lane_s >= PLAIN_QK_DIM) & (lane_s < PLAIN_QK_DIM + ROTARY_DIM)
        rows = slice(hf * hrow, (hf + 1) * hrow)
        latent_rows = ckn[rows, :]
        pieces = []
        for t in range(4 * hf, 4 * hf + 4):
            packed = krx[block, STEP * t : STEP * t + STEP, :].astype(f32)
            for j in range(4):
                moved = pltpu.roll(packed, (192 - 32 * j) % 128, 1)
                pieces.append(jnp.where(on_rope, moved, 0.0))
        rope_key = jnp.concatenate(pieces, axis=0)
        rope_odd = pltpu.roll(rope_key, 64, 1)
        keys = jnp.dot(latent_rows, wku[...], preferred_element_type=f32)
        vals = jnp.dot(latent_rows, wvu[...], preferred_element_type=f32)
        for hp in range(heads // 2):
            cols = slice(128 * hp, 128 * hp + 128)
            k2, v2 = keys[:, cols], vals[:, cols]
            even, odd = slot * heads + 2 * hp, slot * heads + 2 * hp + 1
            kb[even, rows, :] = jnp.where(lane_h < 64, k2, rope_key).astype(bf16)
            kb[odd, rows, :] = jnp.where(lane_h < 64, rope_odd, k2).astype(bf16)
            vb[even, rows, :] = jnp.where(lane_h < 64, v2, ones).astype(bf16)
            vb[odd, rows, :] = jnp.where(lane_h < 64, ones_odd, v2).astype(bf16)

    def block_at(step):
        below = jnp.minimum(z, spn - 1 - z)
        near_block = jnp.where(lax.rem(step, 2) == 1, z - (step + 1) // 2, z + step // 2)
        past = jnp.where(z < spn - 1 - z, step, spn - 1 - step)
        return jnp.where(step <= 2 * below, near_block, past)

    lane = lanes_of((pair, 128))

    def up_q(b):
        for base in range(0, pair, 64):
            def put(cols, value, base=base):
                cqn[base : base + 64, cols] = value

            rms([cq[r, b, base : base + 64, :] for r in range(4)], qgain_ref, put)
        q_all = jnp.dot(cqn[...], wqu[...], preferred_element_type=f32)
        rows = slice(b * pair, (b + 1) * pair)
        for h in range(heads):
            offset = h * (PLAIN_QK_DIM + ROTARY_DIM)
            tile, shift = offset // 128, offset % 128
            head = q_all[:, 128 * tile : 128 * tile + 128]
            if shift:
                head = pltpu.roll(head, 128 - shift, 1)
                if shift + PLAIN_QK_DIM + ROTARY_DIM > 128:
                    rest = q_all[:, 128 * tile + 128 : 128 * tile + 256]
                    head = jnp.where(
                        lane < 128 - shift, head, pltpu.roll(rest, 128 - shift, 1)
                    )
            head = turned(head, cosv[rows, :], sinv[rows, :])
            if h % 2:
                head = pltpu.roll(head, 64, 1)
            head = head.astype(bf16)
            for which in range(2):
                qh[h, which ^ side, b * own : (b + 1) * own, :] = head[
                    which * own : (which + 1) * own
                ]

    for copy in l_small:
        copy.wait()
    l_qu.wait()
    l_ku.wait()
    l_vu.wait()
    acc[...] = jnp.zeros_like(acc)
    mx[...] = jnp.full(mx.shape, NEGATIVE, f32)
    factor = (PLAIN_QK_DIM + ROTARY_DIM) ** (-0.5) * LOG2E
    blocks = [None] + [block_at(jnp.int32(step)) for step in range(1, spn)]

    spread(blocks[1], 0)
    cq_waits = [cq_a[1], cq_a[0]()]
    relay(z, 0)
    for w in cq_waits:
        w()
    up_q(0)
    forward(1, 0)
    cq_waits = [cq_b[1], cq_b[0]()]
    gathered(z, 0)
    expand_half(z, 0)
    relay(z, 1)
    arrive(blocks[1])
    spread(blocks[2], 0)
    for w in cq_waits:
        w()
    up_q(1)
    gathered(z, 1)
    expand_half(z, 1)
    at_end = jnp.logical_not(jnp.logical_and(has_left, has_right))

    @pl.when(jnp.logical_not(at_end))
    def _():
        arrive(blocks[2])

    def rows_of(ref, h, group):
        return ref[h].reshape(tok, 128) if group is None else ref[h, group]

    def score(h, group, slots):
        return [
            lax.dot_general(
                rows_of(qh, h, group),
                kb[slot * heads + h],
                (((1,), (1,)), ((), ())),
                preferred_element_type=f32,
            )
            for slot in slots
        ]

    def attend(h, scores, group, slots):
        bias = bias_ref[h] * LOG2E
        tiles = []
        for part_scores in scores:
            for c in range(0, seg, 128):
                tile = part_scores[:, c : c + 128] * factor
                tiles.append(tile + bias if c < ctxn else tile)
        best = functools.reduce(jnp.maximum, tiles)
        old = rows_of(mx, h, group)
        new = jnp.maximum(old, jnp.max(best, axis=-1, keepdims=True))
        total = rows_of(acc, h, group) * jnp.exp2(old - new)
        each = seg // 128
        for n, slot in enumerate(slots):
            weights = jnp.concatenate(
                [jnp.exp2(t - new).astype(bf16) for t in tiles[n * each : (n + 1) * each]],
                axis=1,
            )
            total = total + jnp.dot(weights, vb[slot * heads + h], preferred_element_type=f32)
        if group is None:
            mx[h] = new.reshape(2, pair, 128)
            acc[h] = total.reshape(2, pair, 128)
        else:
            mx[h, group] = new
            acc[h, group] = total

    def attend_all(after, group=None, slots=(0,)):
        scores = score(0, group, slots)
        for h in range(heads):
            following = score(h + 1, group, slots) if h + 1 < heads else None
            attend(h, scores, group, slots)
            after(h)
            scores = following

    @pl.loop(1, spn)
    def _(step):
        block = block_at(step)
        final_step = step == spn - 1

        def meanwhile(h):
            if h != RELAY_AFTER:
                return

            for part in range(2):
                relay(block, part)

            @pl.when(step == 1)
            def _():
                @pl.when(at_end)
                def _():
                    arrive(blocks[2])

                forward(2, 0)
                spread(blocks[3], 0)
                arrive(blocks[3])

        @pl.when(jnp.logical_not(final_step))
        def _():
            attend_all(meanwhile)

        @pl.when(final_step)
        def _():
            attend_all(meanwhile, 0)

        for part in range(2):
            gathered(block, part)
        slot = jnp.where(final_step, 1, 0)
        for hf in range(2):
            expand_half(block, hf, slot)

    att_relay, att_near = [], []
    hps = heads // 2
    lane64 = lanes_of((pair, 128)) < VALUE_DIM

    def finish(h, group):
        if h % 2 == 0:
            return
        hp = h // 2
        low, high = acc[h - 1, group], acc[h, group]
        totals = jnp.where(lane64, low[:, VALUE_DIM : VALUE_DIM + 1], high[:, 0:1])
        att[p, hp, side ^ group] = (jnp.where(lane64, low, high) / totals).astype(bf16)
        att_relay.append(
            far(
                lambda slot: att.at[slot, hp, side ^ group],
                lambda slot: att.at[slot, hp, 1 - (side ^ group)],
            )
        )
        att_near.append(near(lambda slot: att.at[slot, hp, side ^ group]))

    attend_all(lambda h: finish(h, 0), 0, (1,))
    attend_all(lambda h: finish(h, 1), 1, (0, 1))

    l_wo.wait()
    half_k = heads * VALUE_DIM * 2

    def project(rows_side, chip):
        joined = jnp.concatenate(
            [att[2 * chip + r, hp, rows_side] for r in range(2) for hp in range(hps)], axis=1
        )
        k_rows = pl.ds(pl.multiple_of(chip * half_k, 128), half_k)
        return jnp.dot(joined, wo[k_rows, :], preferred_element_type=f32)

    for w in att_near:
        w()
    part_other[...] = project(1 - side, side)
    att_far = [r() for r in att_relay[:2]]
    part_self[...] = project(side, side)
    att_far += [r() for r in att_relay[2:hps]]
    for w in att_far:
        w()
    made = (part_other[...] + project(1 - side, 1 - side)).astype(bf16)
    for k in range(2):
        for b in range(2):
            row = b * own + k * half
            po[k, b * half : (b + 1) * half, :] = made[row : row + half]
    final = [
        send(po.at[core], pr.at[p], fresh(), {"tp": p2}),
        send(po.at[1 - core], pr.at[p], fresh(), {"tp": p3}),
    ]
    att_far = [r() for r in att_relay[hps:]]
    for w in att_far:
        w()
    made = (part_self[...] + project(side, 1 - side)).astype(bf16)
    for k in range(2):
        for b in range(2):
            row = b * own + k * half
            po[2 + k, b * half : (b + 1) * half, :] = made[row : row + half]
    close = send(po.at[2 + 1 - core], pr.at[p], fresh(), {"tp": p1})

    def mix(j, source):
        cols = pl.ds(pl.multiple_of(j * modw, 128), modw)
        gate = mod[j, 4:5, :]
        for r in range(0, own, STEP):
            out_ref[r : r + STEP, cols] = (
                lat[p, r : r + STEP, cols].astype(f32)
                + gate * source[r : r + STEP, :].astype(f32)
            ).astype(bf16)

    mix(p, po.at[2 + core])
    close.wait_recv()
    mix(p1, pr.at[p1])
    final[0].wait_recv()
    mix(p2, pr.at[p2])
    final[1].wait_recv()
    mix(p3, pr.at[p3])

    for copy in sends:
        copy.wait_send()
    for part in range(2):
        for kind in range(3):
            swap(z, part, kind).wait_send()

        def drain(o, way, onward, more, step=0):
            for kind in range(3):
                swap(o, part, kind).wait_send()
            if part == 0 and passed_on(step):

                @pl.when(more)
                def _():
                    Hop(o, onward, way, part).wait_send()

        for step in range(spn - 1):
            at_distance(step, functools.partial(drain, step=step))

    @pl.when(has_right)
    def _():
        Hop(z, z + 1, 0, 0).wait_send()

    @pl.when(has_left)
    def _():
        Hop(z, z - 1, 1, 0).wait_send()

    at_far_end(lambda target, way: Hop(z, target, way, 0, target).wait_send())
    at_distances(lambda target, way: Hop(z, target, way, 1, target).wait_send())


def fused_device(
    latents,
    conditions,
    context,
    w_shift,
    w_scale,
    w_gate,
    w_qdown,
    w_kvdown,
    w_rope,
    q_gain,
    latent_norm_gain,
    query_up_weight,
    key_up_weight,
    value_up_weight,
    context_bias,
    w_out,
):
    f32, bf16 = jnp.float32, jnp.bfloat16
    spn = lax.axis_size("sp")
    own, width = latents.shape
    ctxn = context.shape[0]
    tok = 4 * own
    seg = tok + ctxn
    heads = context_bias.shape[0]
    modw = w_shift.shape[1]
    kdim, qcols = w_qdown.shape
    kcols = w_kvdown.shape[1]
    cosine, sine = turn_tables(spn, own)
    hbm = pl.BlockSpec(memory_space=pltpu.HBM)
    V, DMA = pltpu.VMEM, pltpu.SemaphoreType.DMA
    scratch = [
        V(conditions.shape, f32),
        pltpu.SMEM(context_bias.shape, f32),
        V((1,) + q_gain.shape, f32),
        V((1,) + latent_norm_gain.shape, f32),
        V(w_rope.shape[::-1], bf16),
        V((16, conditions.shape[1]), f32),
        V((3,) + w_shift.shape, bf16),
        V((4, own, width), bf16),
        V((ctxn, width), bf16),
        V((seg, width), bf16),
        V((kdim, qcols), bf16),
        V((kdim, kcols + 128), bf16),
        V((spn, 8, modw), f32),
        V((4, 8, modw), f32),
        V((4, 2, 2 * own, qcols), bf16),
        V((spn, 4, seg, kcols), bf16),
        V((spn, seg // 4, 128), bf16),
        V((seg, 128), f32),
        V((seg, 4 * kcols), bf16),
        V((2 * own, 4 * qcols), bf16),
        V(query_up_weight.shape, bf16),
        V(key_up_weight.shape, bf16),
        V(value_up_weight.shape, bf16),
        V(w_out.shape, bf16),
        V((tok, 128), f32),
        V((tok, 128), f32),
        V((heads, 2, 2 * own, 128), bf16),
        V((2 * heads, seg, 128), bf16),
        V((2 * heads, seg, 128), bf16),
        V((heads, 2, 2 * own, 128), f32),
        V((heads, 2, 2 * own, 128), f32),
        V((4, heads // 2, 2, 2 * own, 128), bf16),
        V((4, own, modw), bf16),
        V((4, own, modw), bf16),
        V((seg, 128), f32),
        V((seg, 128), f32),
        V((2 * own, modw), f32),
        V((2 * own, modw), f32),
        DMA((18,)),
        DMA((64,)),
        DMA((64,)),
        DMA((2, 2, 2, spn)),
        DMA((2, 2, spn)),
        DMA((3, 2, spn)),
        DMA((3, 2, spn)),
    ]
    return pl.pallas_call(
        block_kernel,
        out_shape=pltpu.VMEM(latents.shape, bf16),
        in_specs=[hbm] * 18,
        out_specs=pl.BlockSpec(memory_space=pltpu.VMEM),
        scratch_shapes=scratch,
        compiler_params=pltpu.CompilerParams(
            collective_id=0, has_side_effects=True, vmem_limit_bytes=56 * 1024 * 1024
        ),
    )(
        conditions,
        context_bias,
        q_gain[None, :],
        latent_norm_gain[None, :],
        w_rope.T,
        latents,
        context,
        w_shift,
        w_scale,
        w_gate,
        w_qdown,
        w_kvdown,
        query_up_weight,
        key_up_weight,
        value_up_weight,
        w_out,
        jnp.asarray(cosine),
        jnp.asarray(sine),
    )


def on_device(*arrays):
    latents, context, bias = arrays[0], arrays[2], arrays[14]
    fits = (
        lax.axis_size("tp") == 4
        and lax.axis_size("sp") == 4
        and latents.shape[0] % 32 == 0
        and context.shape[0] % 128 == 0
        and latents.shape[0] > 2 * BAND
        and (4 * latents.shape[0] + context.shape[0]) == 512
        and arrays[6].shape[1] == 256
        and arrays[7].shape[1] == 128
        and bias.shape[0] == 8
    )
    return fused_device(*arrays) if fits else plain_device(*arrays)


def solution(mesh):
    in_specs = (
        P(("grp", "sp", "tp"), None),
        P("grp", "sp"),
        P(("grp", "sp"), None),
        P("sp", "tp"),
        P("sp", "tp"),
        P("sp", "tp"),
        P(None, "tp"),
        P(None, "tp"),
        P(),
        P(),
        P(),
        P(None, "tp"),
        P(None, "tp"),
        P(None, "tp"),
        P("tp"),
        P(None, "tp"),
    )
    out_specs = P(("grp", "sp", "tp"), None)
    return jax.shard_map(
        on_device, mesh=mesh, in_specs=in_specs, out_specs=out_specs, check_vma=False
    )
```
